256 devices in a mesh: sp: 16 (over y, x), tp: 16 (over z, core).
Axes of the slice: x: 4, y: 4, z: 8, core: 2. Of those that a mesh axis runs over, the one named last changes fastest.
Arguments:
- skip_stream_entry: bfloat16 [8192, 2048], P(('sp', 'tp')), may hold values from -6 to 6
- result_switch_mapped: bfloat16 [8192, 4096], P('sp', 'tp'), may hold values from -6 to 6
- channel_feed_mapped: bfloat16 [8192, 4096], P('sp', 'tp'), may hold values from -6 to 6
- write_coefficient_mapped: bfloat16 [8192, 2048], P('sp', 'tp'), may hold values from -6 to 6
- emission_coefficient_mapped: bfloat16 [8192, 2048], P('sp', 'tp'), may hold values from -6 to 6
- channel_feed_taps: bfloat16 [5, 4096], P(None, 'tp'), may hold values from -2.5 to 2.5
- write_coefficient_taps: bfloat16 [5, 2048], P(None, 'tp'), may hold values from -2.5 to 2.5
- emission_coefficient_taps: bfloat16 [5, 2048], P(None, 'tp'), may hold values from -2.5 to 2.5
- raw_increments: bfloat16 [2, 64, 8192], P(None, 'tp', 'sp'), may hold values from -6 to 6
- channel_log_fade_speed: float32 [2, 64], P(None, 'tp'), may hold values from -20 to 0
- extra_log_fade: float32 [2, 64, 8192], P(None, 'tp', 'sp'), may hold values from -1 to 0
- cluster_scaling_factor: float32 [4096], P('tp'), may hold values from 0.1 to 1.9
- blend_result_matrix: bfloat16 [4096, 2048], P('tp'), may hold values from -0.09375 to 0.09375
- routing_scaling_factor: float32 [2048], replicated, may hold values from 0.1 to 1.9
- specialist_switch_matrix: bfloat16 [32, 2048, 4096], P('sp', None, 'tp'), may hold values from -0.125 to 0.125
- specialist_widen_matrix: bfloat16 [32, 2048, 4096], P('sp', None, 'tp'), may hold values from -0.125 to 0.125
- specialist_contract_matrix: bfloat16 [32, 4096, 2048], P('sp', 'tp'), may hold values from -0.1875 to 0.1875
- picked_specialists: int32 [8192, 2], P(('sp', 'tp')), may hold values from 0 to 31, all different within a row; in each aligned block of 32 rows (0 to 31, 32 to 63, ...) at most 3 rows name the same one
- router_affinities: float32 [8192, 2], P(('sp', 'tp')), may hold values from 0.1 to 1
Outputs:
- result: bfloat16 [8192, 2048], P(('sp', 'tp'))
The draws below stay inside these ranges and needn't reach their ends.
Inputs may be any that keep to these rules, and one draw needn't show every extreme that they name: `picked_specialists`: each row names 2 different experts. Within the rows of one device (aligned blocks of 32 rows) no expert is named more than 3 times, a bound that some block reaches.
All inputs are finite; a program needn't handle non-finite values.
Results may differ from the reference program's by a relative error of at most 0.02.
Values may be sent and summed in bfloat16 or wider, within the bound.
A program may use at most 64 MiB of HBM per device.

```python
import math
import jax
import jax.numpy as jnp
import numpy as np
from jax import lax

WIDTH = 2048
HEADS = 64
HEAD_DIM = 64
GROUPS = 16
STATE = 128
EXPERT_FF = 4096
CONV_W = 5
BLOCK = 128
TOP = 2
SEQ_DEV = 512
INNER = 4096
SERIES_ITEMS = 8192
ROWS_DEV = 32
EXPERTS = 32
CAPACITY = 3
N_SP = 16
N_TP = 16


def draw_raw_increments(key, part):
    first_key, second_key = jax.random.split(key)
    noise = 0.7 * jax.random.normal(second_key, (2, HEADS, SERIES_ITEMS), jnp.float32)
    shifts = jax.random.uniform(first_key, (2, HEADS, SERIES_ITEMS // SEQ_DEV), jnp.float32, -1.5, 1.0)
    return (noise + jnp.repeat(shifts, SEQ_DEV, axis=2)).astype(jnp.bfloat16)


def draw_channel_log_fade_speed(key, part):
    coin_key, slow_key, fast_key = jax.random.split(key, 3)
    share = 0.5
    slow = jnp.log(jax.random.uniform(slow_key, (2, HEADS), jnp.float32, 0.1, 0.4) / SERIES_ITEMS)
    fast = jnp.log(jax.random.uniform(fast_key, (2, HEADS), jnp.float32, 0.05, 0.12))
    return jnp.where(jax.random.uniform(coin_key, (2, HEADS), jnp.float32) < share, slow, fast)


def draw_extra_log_fade(key, part):
    place_key, depth_key = jax.random.split(key)
    third = SERIES_ITEMS // 3
    offsets = jnp.arange(3, dtype=jnp.int32) * third
    places = offsets[None, None, :] + jax.random.randint(place_key, (2, HEADS, 3), 0, third, dtype=jnp.int32)
    depths = jnp.log(jax.random.uniform(depth_key, (2, HEADS, 3), jnp.float32, 0.5, 0.8))
    positions = jnp.arange(SERIES_ITEMS, dtype=jnp.int32)
    landed = positions[None, None, None, :] == places[..., None]
    return jnp.sum(jnp.where(landed, depths[..., None], 0.0), axis=2)


def level_of(rng, dims, cuts, least, largest):
    level, own = 1.0, jax.random.fold_in(rng, 6)
    for position, blocks in cuts:
        heights = jnp.exp(jax.random.uniform(jax.random.fold_in(own, position), (blocks,), jnp.float32, least / len(cuts), largest / len(cuts)))
        level = level * jnp.repeat(heights, dims[position] // blocks).reshape([-1 if axis == position else 1 for axis in range(len(dims))])
    return level


def shared_out(stream_key, own, number, rows, number_of, top, bound, skew):
    order = jax.random.permutation(stream_key, number_of)
    heavy_load, common = load_shares(number_of, rows * top, bound, skew, True), load_shares(number_of, rows * top, bound, skew, False)
    places = jnp.arange(number_of)

    def named(lengths, offset_by):
        used = int((lengths > 0).sum())
        fixed = max(1, used // 4)
        moved = fixed + (places - fixed + offset_by * (used - fixed)) % max(1, number_of - fixed)
        return jnp.zeros((number_of,), jnp.int32).at[order[jnp.where(places < fixed, places, moved)]].set(jnp.asarray(lengths, jnp.int32))

    lengths = jnp.where(number % 4 == 0, named(heavy_load, number // 4), named(common, number - number // 4 - 1))
    mixed = jax.random.permutation(jax.random.fold_in(own, 3), number_of)
    source_of, sink = mixed[0:number_of // 2 * 2:2], mixed[1:number_of // 2 * 2:2]
    room = jnp.minimum(lengths[source_of] - 1, bound - lengths[sink]) // 2
    room = jnp.where((source_of == order[0]) | (sink == order[0]) | (lengths[sink] == 0), 0, jnp.maximum(room, 0))
    moved = jax.random.randint(jax.random.fold_in(own, 4), (number_of // 2,), 0, 1 << 20) % (room + 1)
    lengths = lengths.at[source_of].add(-moved).at[sink].add(moved)
    members = jnp.searchsorted(jnp.cumsum(lengths), jnp.arange(rows * top), side="right").astype(jnp.int32)
    table = members.reshape(top, rows).T
    table = table[jax.random.permutation(jax.random.fold_in(own, 1), rows)]
    offset_by = jax.random.randint(jax.random.fold_in(own, 2), (rows, 1), 0, top)
    return jnp.take_along_axis(table, (jnp.arange(top)[None, :] + offset_by) % top, axis=1)


def load_shares(number_of, total, most, lean, full):
    weights = [(1 << 20) // math.isqrt(rank ** lean) + 1 for rank in range(1, number_of + 1)]
    largest = most if full else min(most, max(-(-total // number_of), total * weights[0] // sum(weights)))
    least = 1 if total - largest >= number_of - 1 else 0
    holding, spare = [largest] + [least] * (number_of - 1), total - largest - least * (number_of - 1)
    while spare > 0:
        free = [i for i in range(1, number_of) if holding[i] < largest] or [i for i in range(1, number_of) if holding[i] < most]
        whole, left = sum([weights[i] for i in free]), spare
        for i in free:
            addition = min(most - holding[i], max(1, left * weights[i] // whole), spare)
            holding[i] = holding[i] + addition
            spare = spare - addition
    return np.array(holding)


def scatter_about(rng, shape, scale, bound, cuts=(), kind=jnp.bfloat16):
    entries = scale * jax.random.normal(rng, shape, jnp.float32)
    if cuts:
        entries = entries * level_of(rng, shape, cuts, -0.22, 0.18)
    return jnp.clip(entries, -bound, bound).astype(kind)


def setup_inputs(seed: int = 0) -> dict:
    splits = jax.random.split(jax.random.key(seed), 20)
    skip_stream_entry = scatter_about(splits[0], (SERIES_ITEMS, WIDTH), 1.0, 6.0, ((0, 256),))
    result_switch_mapped = scatter_about(splits[1], (SERIES_ITEMS, INNER), 1.0, 6.0, ((0, 16), (1, 16)))
    channel_feed_mapped = scatter_about(splits[2], (SERIES_ITEMS, INNER), 1.0, 6.0, ((0, 16), (1, 16)))
    write_coefficient_mapped = scatter_about(splits[3], (SERIES_ITEMS, GROUPS * STATE), 1.0, 6.0, ((0, 16), (1, 16)))
    emission_coefficient_mapped = scatter_about(splits[4], (SERIES_ITEMS, GROUPS * STATE), 1.0, 6.0, ((0, 16), (1, 16)))
    channel_feed_taps = scatter_about(splits[5], (CONV_W, INNER), CONV_W ** -0.5, 2.5, ((1, 16),))
    write_coefficient_taps = scatter_about(splits[6], (CONV_W, GROUPS * STATE), CONV_W ** -0.5, 2.5, ((1, 16),))
    emission_coefficient_taps = scatter_about(splits[7], (CONV_W, GROUPS * STATE), CONV_W ** -0.5, 2.5, ((1, 16),))
    raw_increments = draw_raw_increments(jax.random.fold_in(splits[19], 71), 0)
    channel_log_fade_speed = draw_channel_log_fade_speed(jax.random.fold_in(splits[19], 71), 0)
    extra_log_fade = draw_extra_log_fade(jax.random.fold_in(splits[19], 71), 0)
    cluster_scaling_factor = jnp.clip(1.0 + 0.18 * jax.random.normal(splits[11], (INNER,), jnp.float32), 0.1, 1.9)
    blend_result_matrix = scatter_about(splits[12], (INNER, WIDTH), INNER ** -0.5, 0.09375, ((0, 16),))
    routing_scaling_factor = jnp.clip(1.0 + 0.18 * jax.random.normal(splits[13], (WIDTH,), jnp.float32), 0.1, 1.9)
    specialist_switch_matrix = scatter_about(splits[14], (EXPERTS, WIDTH, EXPERT_FF), WIDTH ** -0.5, 0.125, ((0, 16), (2, 16)))
    specialist_widen_matrix = scatter_about(splits[15], (EXPERTS, WIDTH, EXPERT_FF), WIDTH ** -0.5, 0.125, ((0, 16), (2, 16)))
    specialist_contract_matrix = scatter_about(splits[16], (EXPERTS, EXPERT_FF, WIDTH), (EXPERT_FF // 4) ** -0.5, 0.1875, ((0, 16), (1, 16)))
    picked_specialists_keys = jax.random.split(jax.random.fold_in(splits[17], 1), SERIES_ITEMS // ROWS_DEV)
    picked_specialists_turns = jax.random.permutation(jax.random.fold_in(splits[17], 3), SERIES_ITEMS // ROWS_DEV)
    picked_specialists = jax.vmap(lambda own, number: shared_out(jax.random.fold_in(splits[17], 2), own, number, ROWS_DEV, EXPERTS, TOP, CAPACITY, 1))(picked_specialists_keys, picked_specialists_turns).reshape((SERIES_ITEMS, TOP))
    router_affinities = jnp.clip(jnp.exp(math.log(1.0) - 2.3025851 * jax.random.uniform(splits[18], (SERIES_ITEMS, TOP), jnp.float32) ** level_of(splits[18], (SERIES_ITEMS, TOP), ((0, 256),), -0.2, 0.2)), 0.1, 1.0)
    return dict(skip_stream_entry=skip_stream_entry, result_switch_mapped=result_switch_mapped, channel_feed_mapped=channel_feed_mapped, write_coefficient_mapped=write_coefficient_mapped, emission_coefficient_mapped=emission_coefficient_mapped, channel_feed_taps=channel_feed_taps, write_coefficient_taps=write_coefficient_taps, emission_coefficient_taps=emission_coefficient_taps, raw_increments=raw_increments, channel_log_fade_speed=channel_log_fade_speed, extra_log_fade=extra_log_fade, cluster_scaling_factor=cluster_scaling_factor, blend_result_matrix=blend_result_matrix, routing_scaling_factor=routing_scaling_factor, specialist_switch_matrix=specialist_switch_matrix, specialist_widen_matrix=specialist_widen_matrix, specialist_contract_matrix=specialist_contract_matrix, picked_specialists=picked_specialists, router_affinities=router_affinities)


EPSILON = 1e-06
HIGHEST_MODE = lax.Precision.HIGHEST

def centred_conv(padded, weights, series_count):
    summed = jnp.zeros((series_count, padded.shape[1]), jnp.float32)
    for offset in range(weights.shape[0]):
        summed = summed + weights[offset].astype(jnp.float32) * padded[offset:offset + series_count].astype(jnp.float32)
    return jax.nn.silu(summed)

def local_sweep(inputs, entry_state, readout_state, log_fade_factor, softplus_increment):
    seq_len = inputs.shape[0]
    blocks = seq_len // BLOCK
    heads_here = log_fade_factor.shape[0]
    groups_here = entry_state.shape[1] // STATE
    per_group = heads_here // groups_here
    values = inputs.reshape(blocks, BLOCK, groups_here, per_group, HEAD_DIM)
    b_blocks = entry_state.reshape(blocks, BLOCK, groups_here, STATE)
    c_blocks = readout_state.reshape(blocks, BLOCK, groups_here, STATE)
    decay_blocks = log_fade_factor.reshape(groups_here, per_group, blocks, BLOCK)
    step_blocks = softplus_increment.reshape(groups_here, per_group, blocks, BLOCK)
    cumulative = jnp.cumsum(decay_blocks, axis=-1)
    group_inner = jnp.einsum('bign,bjgn->gbij', c_blocks, b_blocks, precision=HIGHEST_MODE)
    spread = cumulative[..., :, None] - cumulative[..., None, :]
    lower_tri = jnp.arange(BLOCK)[:, None] >= jnp.arange(BLOCK)[None, :]
    mixing = jnp.exp(jnp.where(lower_tri, spread, -jnp.inf)) * step_blocks[..., None, :] * group_inner[:, None]
    within = jnp.einsum('gkbij,bjgkp->bigkp', mixing, values, precision=HIGHEST_MODE)
    to_end = jnp.exp(cumulative[..., -1:] - cumulative) * step_blocks
    block_states = jnp.einsum('gkbj,bjgkp,bjgn->bgkpn', to_end, values, b_blocks, precision=HIGHEST_MODE)
    block_decay = cumulative[..., -1]

    def advance(carried, pieces):
        state_piece, decay_piece = pieces
        return (carried * jnp.exp(decay_piece)[..., None, None] + state_piece, carried)
    zero_state = jnp.zeros((groups_here, per_group, HEAD_DIM, STATE), jnp.float32)
    final_state, entering = lax.scan(advance, zero_state, (block_states, jnp.moveaxis(block_decay, -1, 0)))
    before = jnp.cumsum(block_decay, axis=-1) - block_decay
    return ((within, entering, cumulative, before, c_blocks), (lax.optimization_barrier(jnp.sum(block_decay, axis=-1)), final_state))

def finish_sweep(parts, carried):
    within, entering, cumulative, before, c_blocks = parts
    entering = entering + carried[None] * jnp.exp(jnp.moveaxis(before, -1, 0))[..., None, None]
    readout = jnp.einsum('bign,bgkpn->bigkp', c_blocks, entering, precision=HIGHEST_MODE)
    readout = readout * jnp.exp(jnp.transpose(cumulative, (2, 3, 0, 1)))[..., None]
    combined = within + readout
    return combined.reshape(combined.shape[0] * combined.shape[1], -1)

def blend_parts_list(channel_feed_bordered, write_coefficient_bordered, emission_coefficient_bordered, channel_feed_taps, write_coefficient_taps, emission_coefficient_taps, raw_increments, channel_log_fade_speed, extra_log_fade, series_count):
    inputs = centred_conv(channel_feed_bordered, channel_feed_taps, series_count)
    entry_state = centred_conv(write_coefficient_bordered, write_coefficient_taps, series_count)
    readout_state = centred_conv(emission_coefficient_bordered, emission_coefficient_taps, series_count)
    softplus_increment = jax.nn.softplus(raw_increments.astype(jnp.float32))
    log_fade_factor = -softplus_increment * jnp.exp(channel_log_fade_speed)[..., None] + extra_log_fade
    onward_pass = local_sweep(inputs, entry_state, readout_state, log_fade_factor[0], softplus_increment[0])
    backward_pass = local_sweep(jnp.flip(inputs, 0), jnp.flip(entry_state, 0), jnp.flip(readout_state, 0), jnp.flip(log_fade_factor[1], -1), jnp.flip(softplus_increment[1], -1))
    return (onward_pass, backward_pass)

def gated_norm(mixed_sum, result_switch_mapped, cluster_scaling_factor):
    gated = mixed_sum * jax.nn.silu(result_switch_mapped.astype(jnp.float32))
    grouped = gated.reshape(gated.shape[0], -1, INNER // GROUPS)
    normalized = grouped * lax.rsqrt(lax.optimization_barrier(jnp.mean(grouped * grouped, axis=-1, keepdims=True)) + EPSILON)
    return (normalized.reshape(gated.shape) * cluster_scaling_factor).astype(jnp.bfloat16)

def rms_scale(stream, gain):
    values = stream.astype(jnp.float32)
    return (values * lax.rsqrt(lax.optimization_barrier(jnp.mean(values * values, axis=-1, keepdims=True)) + EPSILON) * gain).astype(jnp.bfloat16)

def reference(skip_stream_entry, result_switch_mapped, channel_feed_mapped, write_coefficient_mapped, emission_coefficient_mapped, channel_feed_taps, write_coefficient_taps, emission_coefficient_taps, raw_increments, channel_log_fade_speed, extra_log_fade, cluster_scaling_factor, blend_result_matrix, routing_scaling_factor, specialist_switch_matrix, specialist_widen_matrix, specialist_contract_matrix, picked_specialists, router_affinities):
    rim_width = CONV_W // 2
    filter_border_width = ((rim_width, rim_width), (0, 0))
    onward_pass, backward_pass = blend_parts_list(jnp.pad(channel_feed_mapped, filter_border_width), jnp.pad(write_coefficient_mapped, filter_border_width), jnp.pad(emission_coefficient_mapped, filter_border_width), channel_feed_taps, write_coefficient_taps, emission_coefficient_taps, raw_increments, channel_log_fade_speed, extra_log_fade, SERIES_ITEMS)
    zero_carry = jnp.zeros_like(onward_pass[1][1])
    mixed_sum = finish_sweep(onward_pass[0], zero_carry) + jnp.flip(finish_sweep(backward_pass[0], zero_carry), 0)
    mixed_rows = gated_norm(mixed_sum, result_switch_mapped, cluster_scaling_factor)
    slice_width = INNER // N_TP

    def add_slice(summed, slice_index):
        columns = lax.dynamic_slice_in_dim(mixed_rows, slice_index * slice_width, slice_width, 1)
        weights = lax.dynamic_slice_in_dim(blend_result_matrix, slice_index * slice_width, slice_width, 0)
        partial_sum = jnp.dot(columns, weights, preferred_element_type=jnp.float32).astype(jnp.bfloat16)
        partial_sum = lax.optimization_barrier(partial_sum)
        return (summed + partial_sum.astype(jnp.float32), slice_index)
    projected = lax.scan(add_slice, jnp.zeros((SERIES_ITEMS, WIDTH), jnp.float32), jnp.arange(N_TP, dtype=jnp.int32))[0]
    after_mixer = (skip_stream_entry.astype(jnp.float32) + projected).astype(jnp.bfloat16)
    normed = rms_scale(after_mixer, routing_scaling_factor)
    row_count = SERIES_ITEMS * TOP
    flat_routes = picked_specialists.reshape(row_count)
    owner = jnp.arange(row_count, dtype=jnp.int32) // TOP
    limit = N_SP * N_TP * CAPACITY
    ff_slice = EXPERT_FF // N_TP

    def one_expert(outputs, expert):
        chosen = flat_routes == expert
        chosen_rank = jnp.cumsum(chosen.astype(jnp.int32)) - 1
        target = jnp.where(chosen, chosen_rank, limit)
        member = jnp.zeros((limit,), jnp.int32).at[target].set(jnp.arange(row_count, dtype=jnp.int32), mode='drop')
        filled = jnp.zeros((limit,), jnp.int32).at[target].set(1, mode='drop')
        picked = normed[owner[member]]
        gate_part = jnp.dot(picked, specialist_switch_matrix[expert], preferred_element_type=jnp.float32)
        up_part = jnp.dot(picked, specialist_widen_matrix[expert], preferred_element_type=jnp.float32)
        hidden = (jax.nn.silu(gate_part) * up_part).astype(jnp.bfloat16)
        pieces = jnp.einsum('rsf,sfd->rsd', hidden.reshape(limit, N_TP, ff_slice).astype(jnp.float32), specialist_contract_matrix[expert].reshape(N_TP, ff_slice, WIDTH).astype(jnp.float32))
        pieces = lax.optimization_barrier(pieces.astype(jnp.bfloat16))
        expert_out = lax.optimization_barrier(jnp.sum(pieces.astype(jnp.float32), axis=1)).astype(jnp.bfloat16)
        destination = jnp.where(filled > 0, member, row_count)
        return (outputs.at[destination].set(expert_out, mode='drop'), expert)
    assigned = lax.scan(one_expert, jnp.zeros((row_count, WIDTH), jnp.bfloat16), jnp.arange(EXPERTS, dtype=jnp.int32))[0]
    weights = router_affinities / lax.optimization_barrier(jnp.sum(router_affinities, axis=-1, keepdims=True))
    mixture = lax.optimization_barrier(jnp.sum(weights[..., None] * assigned.reshape(SERIES_ITEMS, TOP, WIDTH).astype(jnp.float32), axis=1))
    return (after_mixer.astype(jnp.float32) + mixture).astype(jnp.bfloat16)
```

```python
import math

import jax
import jax.numpy as jnp
from jax import lax
from jax.experimental import pallas as pl
from jax.experimental.pallas import tpu as pltpu
from jax.sharding import PartitionSpec as P

WIDTH = 2048
HEAD_DIM = 64
GROUPS = 16
STATE = 128
CONV_W = 5
BLOCK = 128
TOP = 2
INNER = 4096


EPSILON = 1e-06


def with_halo(block, sides, width):
    for axis, dim in sides:
        count = lax.axis_size(axis)
        forward = [(i, i + 1) for i in range(count - 1)]
        backward = [(target, source) for source, target in forward]
        low = lax.ppermute(
            lax.slice_in_dim(block, block.shape[dim] - width, None, axis=dim), axis, forward
        )
        high = lax.ppermute(lax.slice_in_dim(block, 0, width, axis=dim), axis, backward)
        block = jnp.concatenate([low, block, high], axis=dim)
    return block


def in_one_piece(arrays, axis, dim, along):
    widths = [math.prod(a.shape[along:]) for a in arrays]
    both = jnp.concatenate(
        [a.reshape(*a.shape[:along], w) for a, w in zip(arrays, widths)], axis=along
    )
    filled = lax.all_gather(both, axis, axis=dim, tiled=True)
    parts = jnp.split(filled, [sum(widths[:k]) for k in range(1, len(widths))], axis=along)
    return tuple(
        (b.reshape(*filled.shape[:along], *a.shape[along:]) for a, b in zip(arrays, parts))
    )


def split_up(shard, dim, peers):
    dims = shard.shape
    parts = shard.reshape(*dims[:dim], peers, dims[dim] // peers, *dims[dim + 1 :])
    return jnp.moveaxis(parts, dim, 0)


def summed_on_arrival(shard, axis, dim):
    parts = split_up(shard, dim, lax.axis_size(axis))
    arrived = lax.all_to_all(parts, axis, split_axis=0, concat_axis=0, tiled=True)
    return arrived.astype(jnp.float32).sum(axis=0)


def centred_conv(padded, weights, series_count):
    summed = jnp.zeros((series_count, padded.shape[1]), jnp.float32)
    for offset in range(weights.shape[0]):
        summed = summed + weights[offset].astype(jnp.float32) * padded[
            offset : offset + series_count
        ].astype(jnp.float32)
    return jax.nn.silu(summed)


def local_sweep(inputs, entry_state, readout_state, log_fade_factor, softplus_increment):
    seq_len = inputs.shape[0]
    blocks = seq_len // BLOCK
    heads_here = log_fade_factor.shape[0]
    groups_here = entry_state.shape[1] // STATE
    per_group = heads_here // groups_here
    values = inputs.reshape(blocks, BLOCK, groups_here, per_group, HEAD_DIM)
    b_blocks = entry_state.reshape(blocks, BLOCK, groups_here, STATE)
    c_blocks = readout_state.reshape(blocks, BLOCK, groups_here, STATE)
    decay_blocks = log_fade_factor.reshape(groups_here, per_group, blocks, BLOCK)
    step_blocks = softplus_increment.reshape(groups_here, per_group, blocks, BLOCK)
    cumulative = jnp.cumsum(decay_blocks, axis=-1)
    group_inner = jnp.einsum("bign,bjgn->gbij", c_blocks, b_blocks)
    spread = cumulative[..., :, None] - cumulative[..., None, :]
    lower_tri = jnp.arange(BLOCK)[:, None] >= jnp.arange(BLOCK)[None, :]
    mixing = (
        jnp.exp(jnp.where(lower_tri, spread, -jnp.inf))
        * step_blocks[..., None, :]
        * group_inner[:, None]
    )
    within = jnp.einsum("gkbij,bjgkp->bigkp", mixing, values)
    to_end = jnp.exp(cumulative[..., -1:] - cumulative) * step_blocks
    block_states = jnp.einsum("gkbj,bjgkp,bjgn->bgkpn", to_end, values, b_blocks)
    block_decay = cumulative[..., -1]

    def advance(carried, pieces):
        state_piece, decay_piece = pieces
        return (carried * jnp.exp(decay_piece)[..., None, None] + state_piece, carried)

    zero_state = jnp.zeros((groups_here, per_group, HEAD_DIM, STATE), jnp.float32)
    final_state, entering = lax.scan(
        advance, zero_state, (block_states, jnp.moveaxis(block_decay, -1, 0))
    )
    before = jnp.cumsum(block_decay, axis=-1) - block_decay
    return (
        (within, entering, cumulative, before, c_blocks),
        (jnp.sum(block_decay, axis=-1), final_state),
    )


def finish_sweep(parts, carried):
    within, entering, cumulative, before, c_blocks = parts
    entering = entering + carried[None] * jnp.exp(jnp.moveaxis(before, -1, 0))[..., None, None]
    readout = jnp.einsum("bign,bgkpn->bigkp", c_blocks, entering)
    readout = readout * jnp.exp(jnp.transpose(cumulative, (2, 3, 0, 1)))[..., None]
    combined = within + readout
    return combined.reshape(combined.shape[0] * combined.shape[1], -1)


def blend_parts_list(
    channel_feed_bordered,
    write_coefficient_bordered,
    emission_coefficient_bordered,
    channel_feed_taps,
    write_coefficient_taps,
    emission_coefficient_taps,
    raw_increments,
    channel_log_fade_speed,
    extra_log_fade,
    series_count,
):
    inputs = centred_conv(channel_feed_bordered, channel_feed_taps, series_count)
    entry_state = centred_conv(write_coefficient_bordered, write_coefficient_taps, series_count)
    readout_state = centred_conv(
        emission_coefficient_bordered, emission_coefficient_taps, series_count
    )
    softplus_increment = jax.nn.softplus(raw_increments.astype(jnp.float32))
    log_fade_factor = (
        -softplus_increment * jnp.exp(channel_log_fade_speed)[..., None] + extra_log_fade
    )
    onward_pass = local_sweep(
        inputs, entry_state, readout_state, log_fade_factor[0], softplus_increment[0]
    )
    backward_pass = local_sweep(
        jnp.flip(inputs, 0),
        jnp.flip(entry_state, 0),
        jnp.flip(readout_state, 0),
        jnp.flip(log_fade_factor[1], -1),
        jnp.flip(softplus_increment[1], -1),
    )
    return (onward_pass, backward_pass)


def gated_norm(mixed_sum, result_switch_mapped, cluster_scaling_factor):
    gated = mixed_sum * jax.nn.silu(result_switch_mapped.astype(jnp.float32))
    grouped = gated.reshape(gated.shape[0], -1, INNER // GROUPS)
    normalized = grouped * lax.rsqrt(jnp.mean(grouped * grouped, axis=-1, keepdims=True) + EPSILON)
    return (normalized.reshape(gated.shape) * cluster_scaling_factor).astype(jnp.bfloat16)


def rms_scale(stream, gain):
    values = stream.astype(jnp.float32)
    return (
        values * lax.rsqrt(jnp.mean(values * values, axis=-1, keepdims=True) + EPSILON) * gain
    ).astype(jnp.bfloat16)


def fold_summaries(gathered, position):
    fwd_totals, fwd_finals, bwd_totals, bwd_finals = gathered
    device_order = jnp.arange(fwd_totals.shape[0], dtype=jnp.int32)[:, None, None]
    earlier = device_order < position
    later_side = device_order > position
    fwd_running = jnp.cumsum(fwd_totals, axis=0)
    fwd_reach = jnp.sum(jnp.where(earlier, fwd_totals, 0.0), axis=0)
    fwd_weight = jnp.exp(jnp.where(earlier, fwd_reach - fwd_running, -jnp.inf))
    bwd_running = jnp.cumsum(bwd_totals, axis=0)
    bwd_reach = jnp.sum(jnp.where(device_order <= position, bwd_totals, 0.0), axis=0)
    bwd_weight = jnp.exp(jnp.where(later_side, bwd_running - bwd_totals - bwd_reach, -jnp.inf))
    carried_fwd = jnp.einsum("jgk,jgkpn->gkpn", fwd_weight, fwd_finals)
    carried_bwd = jnp.einsum("jgk,jgkpn->gkpn", bwd_weight, bwd_finals)
    return (carried_fwd, carried_bwd)


MESH = pl.DeviceIdType.MESH
F32 = jnp.float32
BF16 = jnp.bfloat16
HIGH = lax.Precision.HIGHEST
NZ = 8
NS = 16


def wrap(value, count):
    return lax.rem(value + count, count)


def remote(source, target, send_sem, recv_sem, sp, tp):
    return pltpu.make_async_remote_copy(
        src_ref=source,
        dst_ref=target,
        send_sem=send_sem,
        recv_sem=recv_sem,
        device_id=(sp, tp),
        device_id_type=MESH,
    )


def matmul(left, right):
    return jnp.dot(left, right, preferred_element_type=F32)


def greet(peers_tp, over_sp):
    s, t = lax.axis_index("sp"), lax.axis_index("tp")
    barrier = pltpu.get_barrier_semaphore()
    for peer in peers_tp:
        pl.semaphore_signal(barrier, inc=1, device_id=(s, peer), device_id_type=MESH)
    count = len(peers_tp)
    if over_sp:

        def signal_peer(k, carry):
            pl.semaphore_signal(
                barrier, inc=1, device_id=(lax.rem(s + k, NS), t), device_id_type=MESH
            )
            return carry

        lax.fori_loop(1, NS, signal_peer, 0)
        count += NS - 1
    pl.semaphore_wait(barrier, count)


def ring_reduce(partial, landing4, landing3, send_sems, recv_sems, z, c, s):
    up, down = 2 * wrap(z + 1, NZ) + c, 2 * wrap(z - 1, NZ) + c

    def piece(chain, half, k):
        downward = (chain == 0) == (half == 0)
        hops = 4 if chain == 0 else 3
        dest = wrap(z - hops + k, NZ) if downward else lax.rem(z + hops - k, NZ)
        landing = landing4 if chain == 0 else landing3
        sem = (0 if chain == 0 else 8) + 4 * half + k
        copy = remote(
            partial.at[dest, half],
            landing.at[half, k],
            send_sems.at[sem],
            recv_sems.at[sem],
            s,
            down if downward else up,
        )
        return dest, landing, copy

    def add(dest, half, landing, k):
        total = partial[dest, half].astype(F32) + landing[half, k].astype(F32)
        partial[dest, half] = total.astype(BF16)

    order = ((0, 0), (0, 1), (1, 0), (1, 1))
    sent = []
    for k in range(5):
        for chain, half in order:
            hops = 4 if chain == 0 else 3
            if k > hops:
                continue
            if k > 0:
                _, landing, before = piece(chain, half, k - 1)
                before.wait_recv()
                if k < hops:
                    dest, _, _ = piece(chain, half, k)
                else:
                    dest = z
                add(dest, half, landing, k - 1)
            if k < hops:
                _, _, copy = piece(chain, half, k)
                copy.start()
                sent.append(copy)
    for copy in sent:
        copy.wait_send()


def moe_kernel(
    normed_ref,
    after_ref,
    picks_ref,
    affinity_ref,
    gate_hbm,
    up_hbm,
    down_hbm,
    out_ref,
    tokens,
    weighed,
    gate_w,
    up_w,
    down_w,
    slots,
    arrived,
    back,
    rows,
    results,
    landing4,
    landing3,
    contribution,
    incoming,
    local_sems,
    pair_send,
    pair_recv,
    sp_send,
    sp_recv,
    gather_send,
    gather_recv,
    reduce_send,
    reduce_recv,
    back_send,
    back_recv,
):
    s, t = lax.axis_index("sp"), lax.axis_index("tp")
    z, c = t // 2, lax.rem(t, 2)
    other = 2 * z + (1 - c)
    up, down = 2 * wrap(z + 1, NZ) + c, 2 * wrap(z - 1, NZ) + c

    loads = [
        pltpu.make_async_copy(source.at[c], target.at[0], local_sems.at[k])
        for k, (source, target) in enumerate(
            ((gate_hbm, gate_w), (up_hbm, up_w), (down_hbm, down_w))
        )
    ]
    for load in loads:
        load.start()

    greet((other, up, down), True)

    expert_lane = lax.broadcasted_iota(jnp.int32, (32, 128), 1)
    share = affinity_ref[...]
    share = share / jnp.sum(share, axis=-1, keepdims=True)
    own = jnp.where(picks_ref[:, 0:1] == expert_lane, share[:, 0:1], 0.0) + jnp.where(
        picks_ref[:, 1:2] == expert_lane, share[:, 1:2], 0.0
    )
    weighed[c] = own
    tokens[c] = normed_ref[...]
    pair = [
        remote(weighed.at[c], weighed.at[c], pair_send.at[0], pair_recv.at[0], s, other),
        remote(normed_ref, tokens.at[c], pair_send.at[1], pair_recv.at[1], s, other),
        remote(gate_hbm.at[1 - c], gate_w.at[1], pair_send.at[2], pair_recv.at[2], s, other),
        remote(up_hbm.at[1 - c], up_w.at[1], pair_send.at[3], pair_recv.at[3], s, other),
        remote(down_hbm.at[1 - c], down_w.at[1], pair_send.at[4], pair_recv.at[4], s, other),
    ]
    for copy in pair:
        copy.start()
    pair[0].wait_recv()
    pair[1].wait_recv()

    weight = weighed[...].reshape(64, 128)
    named = jnp.where(weight > 0.0, 1.0, 0.0)
    token_row = lax.broadcasted_iota(jnp.int32, (64, 64), 0)
    token_col = lax.broadcasted_iota(jnp.int32, (64, 64), 1)
    earlier = jnp.where(
        (token_col < token_row) & ((token_col >= 32) == (token_row >= 32)), 1.0, 0.0
    )
    rank = matmul(earlier.astype(BF16), named.astype(BF16))
    lane_e = lax.broadcasted_iota(jnp.int32, (128, 128), 0)
    slot_lane = lax.broadcasted_iota(jnp.int32, (128, 128), 1)
    spread = jnp.where(lane_e == 2 * (slot_lane // 8) + c, 1.0, 0.0)
    place = lax.rem(lax.broadcasted_iota(jnp.int32, (64, 128), 1), 8)
    second = jnp.where(place >= 3, 1, 0)
    token_core = jnp.where(lax.broadcasted_iota(jnp.int32, (64, 128), 0) >= 32, 1, 0)
    wanted = (place - 3 * second).astype(F32)
    named_slot = matmul(named.astype(BF16), spread.astype(BF16))
    rank_slot = matmul(rank.astype(BF16), spread.astype(BF16))
    chosen = (
        (named_slot > 0.5) & (jnp.abs(rank_slot - wanted) < 0.5) & (token_core == second)
        & (place < 6)
    )
    onehot = jnp.where(chosen, 1.0, 0.0)
    weight_slot = jnp.where(
        chosen, jnp.dot(weight, spread, precision=HIGH, preferred_element_type=F32), 0.0
    )
    everything = tokens[...].reshape(64, WIDTH)
    filled = matmul(onehot.T.astype(BF16), everything)
    slots[...] = filled.reshape(NS, 8, WIDTH).astype(BF16)

    def send_slots(k, carry):
        peer = lax.rem(s + k, NS)
        remote(slots.at[peer], arrived.at[s], sp_send.at[k], sp_recv.at[k], peer, t).start()
        return carry

    lax.fori_loop(1, NS, send_slots, 0)
    arrived[s] = slots[s]

    def await_slots(k, carry):
        remote(slots.at[s], arrived.at[s], sp_send.at[k], sp_recv.at[k], s, t).wait_recv()
        return carry

    lax.fori_loop(1, NS, await_slots, 0)

    dense_row = lax.broadcasted_iota(jnp.int32, (96, 128), 0)
    padded_row = lax.broadcasted_iota(jnp.int32, (96, 128), 1)
    dense = jnp.where(padded_row == 8 * (dense_row // 6) + lax.rem(dense_row, 6), 1.0, 0.0)
    padded = arrived[...].astype(F32).reshape(128, WIDTH).astype(BF16)
    packed = matmul(dense.astype(BF16), padded).astype(BF16)
    rows[z] = packed.reshape(2, 48, WIDTH)

    def hop(upward, half, k):
        chunk = wrap(z - k, NZ) if upward else lax.rem(z + k, NZ)
        sem = (0 if upward else 8) + 4 * half + k
        return remote(
            rows.at[chunk, half],
            rows.at[chunk, half],
            gather_send.at[sem],
            gather_recv.at[sem],
            s,
            up if upward else down,
        )

    def arrival(upward, half, k):
        chunk = wrap(z - k - 1, NZ) if upward else lax.rem(z + k + 1, NZ)
        sem = (0 if upward else 8) + 4 * half + k
        return remote(
            rows.at[chunk, half],
            rows.at[chunk, half],
            gather_send.at[sem],
            gather_recv.at[sem],
            s,
            up if upward else down,
        )

    for upward, half in ((True, 0), (False, 1), (True, 1), (False, 0)):
        hop(upward, half, 0).start()
    for load in loads:
        load.wait()
    for copy in pair[2:]:
        copy.wait_recv()

    def step(i, carry):
        k = (i - 1) // 2

        @pl.when(lax.rem(i, 2) == 1)
        def _():
            for upward, half in ((True, 0), (False, 1)):
                arrival(upward, half, k).wait_recv()

                @pl.when(k < 3)
                def _():
                    hop(upward, half, k + 1).start()

            @pl.when(k < 3)
            def _():
                for upward, half in ((True, 1), (False, 0)):
                    arrival(upward, half, k).wait_recv()

                    @pl.when(k < 2)
                    def _():
                        hop(upward, half, k + 1).start()

        shift = (i + 1) // 2
        chunk = jnp.where(lax.rem(i, 2) == 1, wrap(z - shift, NZ), lax.rem(z + shift, NZ))
        x = rows[chunk].reshape(96, WIDTH)
        total = None
        for part in range(2):
            gate = matmul(x, gate_w[part])
            wide = matmul(x, up_w[part])
            hidden = (gate * jax.nn.sigmoid(gate) * wide).astype(BF16)
            piece = matmul(hidden, down_w[part])
            total = piece if total is None else total + piece
        results[chunk] = total.astype(BF16).reshape(2, 48, WIDTH)
        return carry

    lax.fori_loop(0, 8, step, 0)
    for upward in (True, False):
        for half in (0, 1):
            for k in range(4 if upward == (half == 0) else 3):
                hop(upward, half, k).wait_send()

    ring_reduce(results, landing4, landing3, reduce_send, reduce_recv, z, c, s)

    def end_slots(k, carry):
        remote(slots.at[s], arrived.at[s], sp_send.at[k], sp_recv.at[k], s, t).wait_send()
        return carry

    lax.fori_loop(1, NS, end_slots, 0)
    for copy in pair:
        copy.wait_send()

    reduced = results[z].reshape(96, WIDTH)
    opened = matmul(dense.T.astype(BF16), reduced)
    slots[...] = opened.reshape(NS, 8, WIDTH).astype(BF16)

    def send_back(k, carry):
        peer = lax.rem(s + k, NS)
        remote(slots.at[peer], back.at[s], back_send.at[k], back_recv.at[k], peer, t).start()
        return carry

    lax.fori_loop(1, NS, send_back, 0)
    back[s] = slots[s]

    def await_back(k, carry):
        remote(slots.at[s], back.at[s], back_send.at[k], back_recv.at[k], s, t).wait_recv()
        return carry

    lax.fori_loop(1, NS, await_back, 0)
    answers = back[...].astype(F32).reshape(128, WIDTH).astype(BF16)
    high = weight_slot.astype(BF16)
    low = (weight_slot - high.astype(F32)).astype(BF16)
    mixture = matmul(high, answers) + matmul(low, answers)
    contribution[...] = mixture.reshape(2, 32, WIDTH)
    swap = remote(contribution.at[1 - c], incoming, pair_send.at[5], pair_recv.at[5], s, other)
    swap.start()
    kept = contribution[c] + after_ref[...].astype(F32)
    swap.wait_recv()
    out_ref[...] = (kept + incoming[...]).astype(BF16)
    swap.wait_send()

    def end_back(k, carry):
        remote(slots.at[s], back.at[s], back_send.at[k], back_recv.at[k], s, t).wait_send()
        return carry

    lax.fori_loop(1, NS, end_back, 0)


def moe(normed, after, picks, affinity, gate, up, down):
    vmem = pl.BlockSpec(memory_space=pltpu.VMEM)
    hbm = pl.BlockSpec(memory_space=pl.ANY)
    dma = pltpu.SemaphoreType.DMA
    return pl.pallas_call(
        moe_kernel,
        out_shape=jax.ShapeDtypeStruct((32, WIDTH), BF16),
        in_specs=[vmem] * 4 + [hbm] * 3,
        out_specs=vmem,
        scratch_shapes=[
            pltpu.VMEM((2, 32, WIDTH), BF16),
            pltpu.VMEM((2, 32, 128), F32),
            pltpu.VMEM((2, WIDTH, 256), BF16),
            pltpu.VMEM((2, WIDTH, 256), BF16),
            pltpu.VMEM((2, 256, WIDTH), BF16),
            pltpu.VMEM((NS, 8, WIDTH), BF16),
            pltpu.VMEM((NS, 8, WIDTH), BF16),
            pltpu.VMEM((NS, 8, WIDTH), BF16),
            pltpu.VMEM((NZ, 2, 48, WIDTH), BF16),
            pltpu.VMEM((NZ, 2, 48, WIDTH), BF16),
            pltpu.VMEM((2, 4, 48, WIDTH), BF16),
            pltpu.VMEM((2, 3, 48, WIDTH), BF16),
            pltpu.VMEM((2, 32, WIDTH), F32),
            pltpu.VMEM((32, WIDTH), F32),
            dma((3,)),
            dma((6,)),
            dma((6,)),
            dma((NS,)),
            dma((NS,)),
            dma((16,)),
            dma((16,)),
            dma((16,)),
            dma((16,)),
            dma((NS,)),
            dma((NS,)),
        ],
        compiler_params=pltpu.CompilerParams(
            collective_id=0, has_side_effects=True, vmem_limit_bytes=56 * 1024 * 1024
        ),
    )(normed, after, picks, affinity, gate, up, down)


def per_device(
    skip_stream_entry,
    result_switch_mapped,
    channel_feed_mapped,
    write_coefficient_mapped,
    emission_coefficient_mapped,
    channel_feed_taps,
    write_coefficient_taps,
    emission_coefficient_taps,
    raw_increments,
    channel_log_fade_speed,
    extra_log_fade,
    cluster_scaling_factor,
    blend_result_matrix,
    routing_scaling_factor,
    specialist_switch_matrix,
    specialist_widen_matrix,
    specialist_contract_matrix,
    picked_specialists,
    router_affinities,
):
    series_count = channel_feed_mapped.shape[0]
    rim_width = CONV_W // 2
    sources = (channel_feed_mapped, write_coefficient_mapped, emission_coefficient_mapped)
    edges = jnp.concatenate(
        [jnp.concatenate([source[:rim_width], source[-rim_width:]], 0) for source in sources], 1
    )
    rimmed = with_halo(edges, (("sp", 0),), rim_width)
    padded_list = []
    column_start = 0
    for source in sources:
        width_here = source.shape[1]
        upper_rim = rimmed[:rim_width, column_start : column_start + width_here]
        lower_rim = rimmed[-rim_width:, column_start : column_start + width_here]
        padded_list.append(jnp.concatenate([upper_rim, source, lower_rim], 0))
        column_start = column_start + width_here
    onward_pass, backward_pass = blend_parts_list(
        padded_list[0],
        padded_list[1],
        padded_list[2],
        channel_feed_taps,
        write_coefficient_taps,
        emission_coefficient_taps,
        raw_increments,
        channel_log_fade_speed,
        extra_log_fade,
        series_count,
    )
    fwd_total, fwd_final = onward_pass[1]
    bwd_total, bwd_final = backward_pass[1]
    gathered = tuple(
        (
            part.astype(jnp.float32)
            for part in in_one_piece(
                (
                    fwd_total[None].astype(jnp.bfloat16),
                    fwd_final[None].astype(jnp.bfloat16),
                    bwd_total[None].astype(jnp.bfloat16),
                    bwd_final[None].astype(jnp.bfloat16),
                ),
                "sp",
                0,
                3,
            )
        )
    )
    carried_fwd, carried_bwd = fold_summaries(gathered, lax.axis_index("sp"))
    mixed_sum = finish_sweep(onward_pass[0], carried_fwd) + jnp.flip(
        finish_sweep(backward_pass[0], carried_bwd), 0
    )
    mixed_rows = gated_norm(mixed_sum, result_switch_mapped, cluster_scaling_factor)
    rows_here = skip_stream_entry.shape[0]
    projected = summed_on_arrival(
        jnp.dot(mixed_rows, blend_result_matrix, preferred_element_type=jnp.float32).astype(
            jnp.bfloat16
        ),
        "tp",
        0,
    )
    after_mixer = (skip_stream_entry.astype(jnp.float32) + projected).astype(jnp.bfloat16)
    normed = rms_scale(after_mixer, routing_scaling_factor)
    return moe(
        normed,
        after_mixer,
        picked_specialists,
        router_affinities,
        specialist_switch_matrix,
        specialist_widen_matrix,
        specialist_contract_matrix,
    )


def solution(mesh):
    in_specs = (
        P(("sp", "tp"), None),
        P("sp", "tp"),
        P("sp", "tp"),
        P("sp", "tp"),
        P("sp", "tp"),
        P(None, "tp"),
        P(None, "tp"),
        P(None, "tp"),
        P(None, "tp", "sp"),
        P(None, "tp"),
        P(None, "tp", "sp"),
        P("tp"),
        P("tp", None),
        P(),
        P("sp", None, "tp"),
        P("sp", None, "tp"),
        P("sp", "tp", None),
        P(("sp", "tp"), None),
        P(("sp", "tp"), None),
    )
    out_specs = P(("sp", "tp"), None)
    return jax.shard_map(
        per_device, mesh=mesh, in_specs=in_specs, out_specs=out_specs, check_vma=False
    )
```

```python
import math

import jax
import jax.numpy as jnp
from jax import lax
from jax.experimental import pallas as pl
from jax.experimental.pallas import tpu as pltpu
from jax.sharding import PartitionSpec as P

WIDTH = 2048
HEAD_DIM = 64
GROUPS = 16
STATE = 128
CONV_W = 5
BLOCK = 128
TOP = 2
INNER = 4096


EPSILON = 1e-06


def with_halo(block, sides, width):
    for axis, dim in sides:
        count = lax.axis_size(axis)
        forward = [(i, i + 1) for i in range(count - 1)]
        backward = [(target, source) for source, target in forward]
        low = lax.ppermute(
            lax.slice_in_dim(block, block.shape[dim] - width, None, axis=dim), axis, forward
        )
        high = lax.ppermute(lax.slice_in_dim(block, 0, width, axis=dim), axis, backward)
        block = jnp.concatenate([low, block, high], axis=dim)
    return block


def in_one_piece(arrays, axis, dim, along):
    widths = [math.prod(a.shape[along:]) for a in arrays]
    both = jnp.concatenate(
        [a.reshape(*a.shape[:along], w) for a, w in zip(arrays, widths)], axis=along
    )
    filled = lax.all_gather(both, axis, axis=dim, tiled=True)
    parts = jnp.split(filled, [sum(widths[:k]) for k in range(1, len(widths))], axis=along)
    return tuple(
        (b.reshape(*filled.shape[:along], *a.shape[along:]) for a, b in zip(arrays, parts))
    )


def centred_conv(padded, weights, series_count):
    summed = jnp.zeros((series_count, padded.shape[1]), jnp.float32)
    for offset in range(weights.shape[0]):
        summed = summed + weights[offset].astype(jnp.float32) * padded[
            offset : offset + series_count
        ].astype(jnp.float32)
    return jax.nn.silu(summed)


def local_sweep(inputs, entry_state, readout_state, log_fade_factor, softplus_increment):
    seq_len = inputs.shape[0]
    blocks = seq_len // BLOCK
    heads_here = log_fade_factor.shape[0]
    groups_here = entry_state.shape[1] // STATE
    per_group = heads_here // groups_here
    values = inputs.reshape(blocks, BLOCK, groups_here, per_group, HEAD_DIM)
    b_blocks = entry_state.reshape(blocks, BLOCK, groups_here, STATE)
    c_blocks = readout_state.reshape(blocks, BLOCK, groups_here, STATE)
    decay_blocks = log_fade_factor.reshape(groups_here, per_group, blocks, BLOCK)
    step_blocks = softplus_increment.reshape(groups_here, per_group, blocks, BLOCK)
    cumulative = jnp.cumsum(decay_blocks, axis=-1)
    group_inner = jnp.einsum("bign,bjgn->gbij", c_blocks, b_blocks)
    spread = cumulative[..., :, None] - cumulative[..., None, :]
    lower_tri = jnp.arange(BLOCK)[:, None] >= jnp.arange(BLOCK)[None, :]
    mixing = (
        jnp.exp(jnp.where(lower_tri, spread, -jnp.inf))
        * step_blocks[..., None, :]
        * group_inner[:, None]
    )
    within = jnp.einsum("gkbij,bjgkp->bigkp", mixing, values)
    to_end = jnp.exp(cumulative[..., -1:] - cumulative) * step_blocks
    block_states = jnp.einsum("gkbj,bjgkp,bjgn->bgkpn", to_end, values, b_blocks)
    block_decay = cumulative[..., -1]

    def advance(carried, pieces):
        state_piece, decay_piece = pieces
        return (carried * jnp.exp(decay_piece)[..., None, None] + state_piece, carried)

    zero_state = jnp.zeros((groups_here, per_group, HEAD_DIM, STATE), jnp.float32)
    final_state, entering = lax.scan(
        advance, zero_state, (block_states, jnp.moveaxis(block_decay, -1, 0))
    )
    before = jnp.cumsum(block_decay, axis=-1) - block_decay
    return (
        (within, entering, cumulative, before, c_blocks),
        (jnp.sum(block_decay, axis=-1), final_state),
    )


def finish_sweep(parts, carried):
    within, entering, cumulative, before, c_blocks = parts
    entering = entering + carried[None] * jnp.exp(jnp.moveaxis(before, -1, 0))[..., None, None]
    readout = jnp.einsum("bign,bgkpn->bigkp", c_blocks, entering)
    readout = readout * jnp.exp(jnp.transpose(cumulative, (2, 3, 0, 1)))[..., None]
    combined = within + readout
    return combined.reshape(combined.shape[0] * combined.shape[1], -1)


def blend_parts_list(
    channel_feed_bordered,
    write_coefficient_bordered,
    emission_coefficient_bordered,
    channel_feed_taps,
    write_coefficient_taps,
    emission_coefficient_taps,
    raw_increments,
    channel_log_fade_speed,
    extra_log_fade,
    series_count,
):
    inputs = centred_conv(channel_feed_bordered, channel_feed_taps, series_count)
    entry_state = centred_conv(write_coefficient_bordered, write_coefficient_taps, series_count)
    readout_state = centred_conv(
        emission_coefficient_bordered, emission_coefficient_taps, series_count
    )
    softplus_increment = jax.nn.softplus(raw_increments.astype(jnp.float32))
    log_fade_factor = (
        -softplus_increment * jnp.exp(channel_log_fade_speed)[..., None] + extra_log_fade
    )
    onward_pass = local_sweep(
        inputs, entry_state, readout_state, log_fade_factor[0], softplus_increment[0]
    )
    backward_pass = local_sweep(
        jnp.flip(inputs, 0),
        jnp.flip(entry_state, 0),
        jnp.flip(readout_state, 0),
        jnp.flip(log_fade_factor[1], -1),
        jnp.flip(softplus_increment[1], -1),
    )
    return (onward_pass, backward_pass)


def gated_norm(mixed_sum, result_switch_mapped, cluster_scaling_factor):
    gated = mixed_sum * jax.nn.silu(result_switch_mapped.astype(jnp.float32))
    grouped = gated.reshape(gated.shape[0], -1, INNER // GROUPS)
    normalized = grouped * lax.rsqrt(jnp.mean(grouped * grouped, axis=-1, keepdims=True) + EPSILON)
    return (normalized.reshape(gated.shape) * cluster_scaling_factor).astype(jnp.bfloat16)


def fold_summaries(gathered, position):
    fwd_totals, fwd_finals, bwd_totals, bwd_finals = gathered
    device_order = jnp.arange(fwd_totals.shape[0], dtype=jnp.int32)[:, None, None]
    earlier = device_order < position
    later_side = device_order > position
    fwd_running = jnp.cumsum(fwd_totals, axis=0)
    fwd_reach = jnp.sum(jnp.where(earlier, fwd_totals, 0.0), axis=0)
    fwd_weight = jnp.exp(jnp.where(earlier, fwd_reach - fwd_running, -jnp.inf))
    bwd_running = jnp.cumsum(bwd_totals, axis=0)
    bwd_reach = jnp.sum(jnp.where(device_order <= position, bwd_totals, 0.0), axis=0)
    bwd_weight = jnp.exp(jnp.where(later_side, bwd_running - bwd_totals - bwd_reach, -jnp.inf))
    carried_fwd = jnp.einsum("jgk,jgkpn->gkpn", fwd_weight, fwd_finals)
    carried_bwd = jnp.einsum("jgk,jgkpn->gkpn", bwd_weight, bwd_finals)
    return (carried_fwd, carried_bwd)


MESH = pl.DeviceIdType.MESH
F32 = jnp.float32
BF16 = jnp.bfloat16
HIGH = lax.Precision.HIGHEST
NZ = 8
NS = 16


def wrap(value, count):
    return lax.rem(value + count, count)


def remote(source, target, send_sem, recv_sem, sp, tp):
    return pltpu.make_async_remote_copy(
        src_ref=source,
        dst_ref=target,
        send_sem=send_sem,
        recv_sem=recv_sem,
        device_id=(sp, tp),
        device_id_type=MESH,
    )


def matmul(left, right):
    return jnp.dot(left, right, preferred_element_type=F32)


def greet(peers_tp, over_sp):
    s, t = lax.axis_index("sp"), lax.axis_index("tp")
    barrier = pltpu.get_barrier_semaphore()
    for peer in peers_tp:
        pl.semaphore_signal(barrier, inc=1, device_id=(s, peer), device_id_type=MESH)
    count = len(peers_tp)
    if over_sp:

        def signal_peer(k, carry):
            pl.semaphore_signal(
                barrier, inc=1, device_id=(lax.rem(s + k, NS), t), device_id_type=MESH
            )
            return carry

        lax.fori_loop(1, NS, signal_peer, 0)
        count += NS - 1
    pl.semaphore_wait(barrier, count)


def ring_reduce(partial, landing4, landing3, send_sems, recv_sems, z, c, s):
    up, down = 2 * wrap(z + 1, NZ) + c, 2 * wrap(z - 1, NZ) + c

    def dest_of(chain, half, k):
        hops = 4 - chain
        return wrap(z - hops + k, NZ) if chain == half else lax.rem(z + hops - k, NZ)

    def piece(chain, half, k):
        sem = 8 * chain + 4 * half + k
        return remote(
            partial.at[dest_of(chain, half, k), half],
            (landing3 if chain else landing4).at[half, k],
            send_sems.at[sem],
            recv_sems.at[sem],
            s,
            down if chain == half else up,
        )

    sent = []
    for k in range(5):
        for chain, half in ((0, 0), (0, 1), (1, 0), (1, 1)):
            hops = 4 - chain
            if k > hops:
                continue
            if k > 0:
                piece(chain, half, k - 1).wait_recv()
            if k < hops:
                dest = dest_of(chain, half, k)
                if k > 0:
                    landing = landing3 if chain else landing4
                    total = partial[dest, half].astype(F32) + landing[half, k - 1].astype(F32)
                    partial[dest, half] = total.astype(BF16)
                copy = piece(chain, half, k)
                copy.start()
                sent.append(copy)
    for copy in sent:
        copy.wait_send()
    return [
        partial[z, half].astype(F32) + landing4[half, 3].astype(F32) + landing3[half, 2].astype(F32)
        for half in (0, 1)
    ]


def moe_kernel(
    mixed_ref,
    blend_ref,
    skip_ref,
    gain_ref,
    picks_ref,
    affinity_ref,
    gate_hbm,
    up_hbm,
    down_hbm,
    out_ref,
    mixed_in,
    blend_in,
    projected,
    landing4p,
    landing3p,
    after,
    normed,
    tokens,
    weighed,
    gate_w,
    up_w,
    down_w,
    slots,
    arrived,
    back,
    rows,
    results,
    landing4,
    landing3,
    contribution,
    incoming,
    local_sems,
    pair_send,
    pair_recv,
    sp_send,
    sp_recv,
    project_send,
    project_recv,
    gather_send,
    gather_recv,
    reduce_send,
    reduce_recv,
    back_send,
    back_recv,
):
    s, t = lax.axis_index("sp"), lax.axis_index("tp")
    z, c = t // 2, lax.rem(t, 2)
    other = 2 * z + (1 - c)
    up, down = 2 * wrap(z + 1, NZ) + c, 2 * wrap(z - 1, NZ) + c

    loads = [
        pltpu.make_async_copy(source.at[c], target.at[0], local_sems.at[k])
        for k, (source, target) in enumerate(
            ((gate_hbm, gate_w), (up_hbm, up_w), (down_hbm, down_w))
        )
    ]
    for load in loads:
        load.start()

    greet((other, up, down), True)

    expert_lane = lax.broadcasted_iota(jnp.int32, (32, 128), 1)
    share = affinity_ref[...]
    share = share / jnp.sum(share, axis=-1, keepdims=True)
    own = jnp.where(picks_ref[:, 0:1] == expert_lane, share[:, 0:1], 0.0) + jnp.where(
        picks_ref[:, 1:2] == expert_lane, share[:, 1:2], 0.0
    )
    weighed[c] = own
    pair = [
        remote(mixed_ref.at[:, 1 - c], mixed_in, pair_send.at[6], pair_recv.at[6], s, other),
        remote(blend_ref, blend_in, pair_send.at[7], pair_recv.at[7], s, other),
        remote(weighed.at[c], weighed.at[c], pair_send.at[0], pair_recv.at[0], s, other),
        remote(gate_hbm.at[1 - c], gate_w.at[1], pair_send.at[2], pair_recv.at[2], s, other),
        remote(up_hbm.at[1 - c], up_w.at[1], pair_send.at[3], pair_recv.at[3], s, other),
        remote(down_hbm.at[1 - c], down_w.at[1], pair_send.at[4], pair_recv.at[4], s, other),
    ]
    for copy in pair:
        copy.start()

    first = matmul(mixed_ref[:, c].reshape(256, 256), blend_ref[...])
    pair[0].wait_recv()
    pair[1].wait_recv()
    both = first + matmul(mixed_in[...].reshape(256, 256), blend_in[...])
    projected[...] = both.astype(BF16).reshape(NZ, 2, 16, WIDTH)
    summed = ring_reduce(projected, landing4p, landing3p, project_send, project_recv, z, c, s)
    stream = (skip_ref[...].astype(F32) + jnp.concatenate(summed, axis=0)).astype(BF16)
    after[...] = stream
    stream = stream.astype(F32)
    scale = lax.rsqrt(jnp.mean(stream * stream, axis=-1, keepdims=True) + EPSILON)
    normed[...] = (stream * scale * gain_ref[...]).astype(BF16)
    tokens[c] = normed[...]
    swap = remote(normed, tokens.at[c], pair_send.at[1], pair_recv.at[1], s, other)
    swap.start()
    pair[2].wait_recv()
    swap.wait_recv()
    pair.append(swap)

    weight = weighed[...].reshape(64, 128)
    named = jnp.where(weight > 0.0, 1.0, 0.0)
    token_row = lax.broadcasted_iota(jnp.int32, (64, 64), 0)
    token_col = lax.broadcasted_iota(jnp.int32, (64, 64), 1)
    earlier = jnp.where(
        (token_col < token_row) & ((token_col >= 32) == (token_row >= 32)), 1.0, 0.0
    )
    rank = matmul(earlier.astype(BF16), named.astype(BF16))
    lane_e = lax.broadcasted_iota(jnp.int32, (128, 128), 0)
    slot_lane = lax.broadcasted_iota(jnp.int32, (128, 128), 1)
    spread = jnp.where(lane_e == 2 * (slot_lane // 8) + c, 1.0, 0.0)
    place = lax.rem(lax.broadcasted_iota(jnp.int32, (64, 128), 1), 8)
    second = jnp.where(place >= 3, 1, 0)
    token_core = jnp.where(lax.broadcasted_iota(jnp.int32, (64, 128), 0) >= 32, 1, 0)
    wanted = (place - 3 * second).astype(F32)
    named_slot = matmul(named.astype(BF16), spread.astype(BF16))
    rank_slot = matmul(rank.astype(BF16), spread.astype(BF16))
    chosen = (
        (named_slot > 0.5) & (jnp.abs(rank_slot - wanted) < 0.5) & (token_core == second)
        & (place < 6)
    )
    onehot = jnp.where(chosen, 1.0, 0.0)
    weight_slot = jnp.where(
        chosen, jnp.dot(weight, spread, precision=HIGH, preferred_element_type=F32), 0.0
    )
    everything = tokens[...].reshape(64, WIDTH)
    filled = matmul(onehot.T.astype(BF16), everything)
    slots[...] = filled.reshape(NS, 8, WIDTH).astype(BF16)

    def send_slots(k, carry):
        peer = lax.rem(s + k, NS)
        remote(slots.at[peer], arrived.at[s], sp_send.at[k], sp_recv.at[k], peer, t).start()
        return carry

    lax.fori_loop(1, NS, send_slots, 0)
    arrived[s] = slots[s]

    def await_slots(k, carry):
        remote(slots.at[s], arrived.at[s], sp_send.at[k], sp_recv.at[k], s, t).wait_recv()
        return carry

    lax.fori_loop(1, NS, await_slots, 0)

    dense_row = lax.broadcasted_iota(jnp.int32, (96, 128), 0)
    padded_row = lax.broadcasted_iota(jnp.int32, (96, 128), 1)
    dense = jnp.where(padded_row == 8 * (dense_row // 6) + lax.rem(dense_row, 6), 1.0, 0.0)
    padded = arrived[...].astype(F32).reshape(128, WIDTH).astype(BF16)
    packed = matmul(dense.astype(BF16), padded).astype(BF16)
    rows[z] = packed.reshape(2, 48, WIDTH)

    def hop(upward, half, k):
        chunk = wrap(z - k, NZ) if upward else lax.rem(z + k, NZ)
        sem = (0 if upward else 8) + 4 * half + k
        return remote(
            rows.at[chunk, half],
            rows.at[chunk, half],
            gather_send.at[sem],
            gather_recv.at[sem],
            s,
            up if upward else down,
        )

    def arrival(upward, half, k):
        chunk = wrap(z - k - 1, NZ) if upward else lax.rem(z + k + 1, NZ)
        sem = (0 if upward else 8) + 4 * half + k
        return remote(
            rows.at[chunk, half],
            rows.at[chunk, half],
            gather_send.at[sem],
            gather_recv.at[sem],
            s,
            up if upward else down,
        )

    for upward, half in ((True, 0), (False, 1), (True, 1), (False, 0)):
        hop(upward, half, 0).start()
    for load in loads:
        load.wait()
    for copy in pair[3:6]:
        copy.wait_recv()

    def step(i, carry):
        k = (i - 1) // 2

        @pl.when(lax.rem(i, 2) == 1)
        def _():
            for upward, half in ((True, 0), (False, 1)):
                arrival(upward, half, k).wait_recv()

                @pl.when(k < 3)
                def _():
                    hop(upward, half, k + 1).start()

            @pl.when(k < 3)
            def _():
                for upward, half in ((True, 1), (False, 0)):
                    arrival(upward, half, k).wait_recv()

                    @pl.when(k < 2)
                    def _():
                        hop(upward, half, k + 1).start()

        shift = (i + 1) // 2
        chunk = jnp.where(lax.rem(i, 2) == 1, wrap(z - shift, NZ), lax.rem(z + shift, NZ))
        x = rows[chunk].reshape(96, WIDTH)
        total = None
        for part in range(2):
            gate = matmul(x, gate_w[part])
            wide = matmul(x, up_w[part])
            hidden = (gate * jax.nn.sigmoid(gate) * wide).astype(BF16)
            piece = matmul(hidden, down_w[part])
            total = piece if total is None else total + piece
        results[chunk] = total.astype(BF16).reshape(2, 48, WIDTH)
        return carry

    lax.fori_loop(0, 8, step, 0)
    for upward in (True, False):
        for half in (0, 1):
            for k in range(4 if upward == (half == 0) else 3):
                hop(upward, half, k).wait_send()

    summed = ring_reduce(results, landing4, landing3, reduce_send, reduce_recv, z, c, s)

    def end_slots(k, carry):
        remote(slots.at[s], arrived.at[s], sp_send.at[k], sp_recv.at[k], s, t).wait_send()
        return carry

    lax.fori_loop(1, NS, end_slots, 0)
    for copy in pair:
        copy.wait_send()

    reduced = jnp.concatenate([part.astype(BF16) for part in summed], axis=0)
    opened = matmul(dense.T.astype(BF16), reduced)
    slots[...] = opened.reshape(NS, 8, WIDTH).astype(BF16)

    def send_back(k, carry):
        peer = lax.rem(s + k, NS)
        remote(slots.at[peer], back.at[s], back_send.at[k], back_recv.at[k], peer, t).start()
        return carry

    lax.fori_loop(1, NS, send_back, 0)
    back[s] = slots[s]

    def await_back(k, carry):
        remote(slots.at[s], back.at[s], back_send.at[k], back_recv.at[k], s, t).wait_recv()
        return carry

    lax.fori_loop(1, NS, await_back, 0)
    answers = back[...].astype(F32).reshape(128, WIDTH).astype(BF16)
    high = weight_slot.astype(BF16)
    low = (weight_slot - high.astype(F32)).astype(BF16)
    mixture = matmul(high, answers) + matmul(low, answers)
    contribution[...] = mixture.reshape(2, 32, WIDTH)
    swap = remote(contribution.at[1 - c], incoming, pair_send.at[5], pair_recv.at[5], s, other)
    swap.start()
    kept = contribution[c] + after[...].astype(F32)
    swap.wait_recv()
    out_ref[...] = (kept + incoming[...]).astype(BF16)
    swap.wait_send()

    def end_back(k, carry):
        remote(slots.at[s], back.at[s], back_send.at[k], back_recv.at[k], s, t).wait_send()
        return carry

    lax.fori_loop(1, NS, end_back, 0)


def finish_layer(mixed, blend, skip, gain, picks, affinity, gate, up, down):
    vmem = pl.BlockSpec(memory_space=pltpu.VMEM)
    hbm = pl.BlockSpec(memory_space=pl.ANY)
    dma = pltpu.SemaphoreType.DMA
    return pl.pallas_call(
        moe_kernel,
        out_shape=jax.ShapeDtypeStruct((32, WIDTH), BF16),
        in_specs=[vmem] * 6 + [hbm] * 3,
        out_specs=vmem,
        scratch_shapes=[
            pltpu.VMEM((NZ, 32, 256), BF16),
            pltpu.VMEM((256, WIDTH), BF16),
            pltpu.VMEM((NZ, 2, 16, WIDTH), BF16),
            pltpu.VMEM((2, 4, 16, WIDTH), BF16),
            pltpu.VMEM((2, 3, 16, WIDTH), BF16),
            pltpu.VMEM((32, WIDTH), BF16),
            pltpu.VMEM((32, WIDTH), BF16),
            pltpu.VMEM((2, 32, WIDTH), BF16),
            pltpu.VMEM((2, 32, 128), F32),
            pltpu.VMEM((2, WIDTH, 256), BF16),
            pltpu.VMEM((2, WIDTH, 256), BF16),
            pltpu.VMEM((2, 256, WIDTH), BF16),
            pltpu.VMEM((NS, 8, WIDTH), BF16),
            pltpu.VMEM((NS, 8, WIDTH), BF16),
            pltpu.VMEM((NS, 8, WIDTH), BF16),
            pltpu.VMEM((NZ, 2, 48, WIDTH), BF16),
            pltpu.VMEM((NZ, 2, 48, WIDTH), BF16),
            pltpu.VMEM((2, 4, 48, WIDTH), BF16),
            pltpu.VMEM((2, 3, 48, WIDTH), BF16),
            pltpu.VMEM((2, 32, WIDTH), F32),
            pltpu.VMEM((32, WIDTH), F32),
            dma((3,)),
            dma((8,)),
            dma((8,)),
            dma((NS,)),
            dma((NS,)),
            dma((16,)),
            dma((16,)),
            dma((16,)),
            dma((16,)),
            dma((16,)),
            dma((16,)),
            dma((NS,)),
            dma((NS,)),
        ],
        compiler_params=pltpu.CompilerParams(
            collective_id=0, has_side_effects=True, vmem_limit_bytes=56 * 1024 * 1024
        ),
    )(
        mixed.reshape(NZ, 2, 32, 256),
        blend,
        skip,
        gain.reshape(1, WIDTH),
        picks,
        affinity,
        gate,
        up,
        down,
    )


def per_device(
    skip_stream_entry,
    result_switch_mapped,
    channel_feed_mapped,
    write_coefficient_mapped,
    emission_coefficient_mapped,
    channel_feed_taps,
    write_coefficient_taps,
    emission_coefficient_taps,
    raw_increments,
    channel_log_fade_speed,
    extra_log_fade,
    cluster_scaling_factor,
    blend_result_matrix,
    routing_scaling_factor,
    specialist_switch_matrix,
    specialist_widen_matrix,
    specialist_contract_matrix,
    picked_specialists,
    router_affinities,
):
    series_count = channel_feed_mapped.shape[0]
    rim_width = CONV_W // 2
    sources = (channel_feed_mapped, write_coefficient_mapped, emission_coefficient_mapped)
    edges = jnp.concatenate(
        [jnp.concatenate([source[:rim_width], source[-rim_width:]], 0) for source in sources], 1
    )
    rimmed = with_halo(edges, (("sp", 0),), rim_width)
    padded_list = []
    column_start = 0
    for source in sources:
        width_here = source.shape[1]
        upper_rim = rimmed[:rim_width, column_start : column_start + width_here]
        lower_rim = rimmed[-rim_width:, column_start : column_start + width_here]
        padded_list.append(jnp.concatenate([upper_rim, source, lower_rim], 0))
        column_start = column_start + width_here
    onward_pass, backward_pass = blend_parts_list(
        padded_list[0],
        padded_list[1],
        padded_list[2],
        channel_feed_taps,
        write_coefficient_taps,
        emission_coefficient_taps,
        raw_increments,
        channel_log_fade_speed,
        extra_log_fade,
        series_count,
    )
    fwd_total, fwd_final = onward_pass[1]
    bwd_total, bwd_final = backward_pass[1]
    gathered = tuple(
        (
            part.astype(jnp.float32)
            for part in in_one_piece(
                (
                    fwd_total[None].astype(jnp.bfloat16),
                    fwd_final[None].astype(jnp.bfloat16),
                    bwd_total[None].astype(jnp.bfloat16),
                    bwd_final[None].astype(jnp.bfloat16),
                ),
                "sp",
                0,
                3,
            )
        )
    )
    carried_fwd, carried_bwd = fold_summaries(gathered, lax.axis_index("sp"))
    mixed_sum = finish_sweep(onward_pass[0], carried_fwd) + jnp.flip(
        finish_sweep(backward_pass[0], carried_bwd), 0
    )
    mixed_rows = gated_norm(mixed_sum, result_switch_mapped, cluster_scaling_factor)
    return finish_layer(
        mixed_rows,
        blend_result_matrix,
        skip_stream_entry,
        routing_scaling_factor,
        picked_specialists,
        router_affinities,
        specialist_switch_matrix,
        specialist_widen_matrix,
        specialist_contract_matrix,
    )


def solution(mesh):
    in_specs = (
        P(("sp", "tp"), None),
        P("sp", "tp"),
        P("sp", "tp"),
        P("sp", "tp"),
        P("sp", "tp"),
        P(None, "tp"),
        P(None, "tp"),
        P(None, "tp"),
        P(None, "tp", "sp"),
        P(None, "tp"),
        P(None, "tp", "sp"),
        P("tp"),
        P("tp", None),
        P(),
        P("sp", None, "tp"),
        P("sp", None, "tp"),
        P("sp", "tp", None),
        P(("sp", "tp"), None),
        P(("sp", "tp"), None),
    )
    out_specs = P(("sp", "tp"), None)
    return jax.shard_map(
        per_device, mesh=mesh, in_specs=in_specs, out_specs=out_specs, check_vma=False
    )
```

```python
import jax
import jax.numpy as jnp
from jax import lax
from jax.experimental import pallas as pl
from jax.experimental.pallas import tpu as pltpu
from jax.sharding import PartitionSpec as P

WIDTH = 2048
HEAD_DIM = 64
STATE = 128
CONV_W = 5
BLOCK = 128
EPSILON = 1e-06

MESH = pl.DeviceIdType.MESH
F32 = jnp.float32
BF16 = jnp.bfloat16
HIGH = lax.Precision.HIGHEST
NZ = 8
NS = 16


def wrap(value, count):
    return lax.rem(value + count, count)


def remote(source, target, send_sem, recv_sem, sp, tp):
    return pltpu.make_async_remote_copy(
        src_ref=source,
        dst_ref=target,
        send_sem=send_sem,
        recv_sem=recv_sem,
        device_id=(sp, tp),
        device_id_type=MESH,
    )


def matmul(left, right):
    return jnp.dot(left, right, preferred_element_type=F32)


def greet(peers_tp, over_sp):
    s, t = lax.axis_index("sp"), lax.axis_index("tp")
    barrier = pltpu.get_barrier_semaphore()
    for peer in peers_tp:
        pl.semaphore_signal(barrier, inc=1, device_id=(s, peer), device_id_type=MESH)
    count = len(peers_tp)
    if over_sp:

        def signal_peer(k, carry):
            pl.semaphore_signal(
                barrier, inc=1, device_id=(lax.rem(s + k, NS), t), device_id_type=MESH
            )
            return carry

        lax.fori_loop(1, NS, signal_peer, 0)
        count += NS - 1
    pl.semaphore_wait(barrier, count)


def ring_reduce(partial, landing4, landing3, send_sems, recv_sems, z, c, s):
    up, down = 2 * wrap(z + 1, NZ) + c, 2 * wrap(z - 1, NZ) + c

    def dest_of(chain, half, k):
        hops = 4 - chain
        return wrap(z - hops + k, NZ) if chain == half else lax.rem(z + hops - k, NZ)

    def piece(chain, half, k):
        sem = 8 * chain + 4 * half + k
        return remote(
            partial.at[dest_of(chain, half, k), half],
            (landing3 if chain else landing4).at[half, k],
            send_sems.at[sem],
            recv_sems.at[sem],
            s,
            down if chain == half else up,
        )

    sent = []
    for k in range(5):
        for chain, half in ((0, 0), (0, 1), (1, 0), (1, 1)):
            hops = 4 - chain
            if k > hops:
                continue
            if k > 0:
                piece(chain, half, k - 1).wait_recv()
            if k < hops:
                dest = dest_of(chain, half, k)
                if k > 0:
                    landing = landing3 if chain else landing4
                    total = partial[dest, half].astype(F32) + landing[half, k - 1].astype(F32)
                    partial[dest, half] = total.astype(BF16)
                copy = piece(chain, half, k)
                copy.start()
                sent.append(copy)
    for copy in sent:
        copy.wait_send()
    return [
        partial[z, half].astype(F32) + landing4[half, 3].astype(F32) + landing3[half, 2].astype(F32)
        for half in (0, 1)
    ]


def moe_kernel(
    mixed_ref,
    blend_ref,
    skip_ref,
    gain_ref,
    picks_ref,
    affinity_ref,
    gate_hbm,
    up_hbm,
    down_hbm,
    out_ref,
    mixed_in,
    blend_in,
    projected,
    landing4p,
    landing3p,
    after,
    normed,
    tokens,
    weighed,
    gate_w,
    up_w,
    down_w,
    slots,
    arrived,
    back,
    rows,
    results,
    landing4,
    landing3,
    contribution,
    incoming,
    local_sems,
    pair_send,
    pair_recv,
    sp_send,
    sp_recv,
    project_send,
    project_recv,
    gather_send,
    gather_recv,
    reduce_send,
    reduce_recv,
    back_send,
    back_recv,
):
    s, t = lax.axis_index("sp"), lax.axis_index("tp")
    z, c = t // 2, lax.rem(t, 2)
    other = 2 * z + (1 - c)
    up, down = 2 * wrap(z + 1, NZ) + c, 2 * wrap(z - 1, NZ) + c

    loads = [
        pltpu.make_async_copy(source.at[c], target.at[0], local_sems.at[k])
        for k, (source, target) in enumerate(
            ((gate_hbm, gate_w), (up_hbm, up_w), (down_hbm, down_w))
        )
    ]
    for load in loads:
        load.start()

    greet((other, up, down), True)

    expert_lane = lax.broadcasted_iota(jnp.int32, (32, 128), 1)
    share = affinity_ref[...]
    share = share / jnp.sum(share, axis=-1, keepdims=True)
    own = jnp.where(picks_ref[:, 0:1] == expert_lane, share[:, 0:1], 0.0) + jnp.where(
        picks_ref[:, 1:2] == expert_lane, share[:, 1:2], 0.0
    )
    weighed[c] = own
    pair = [
        remote(mixed_ref.at[:, 1 - c], mixed_in, pair_send.at[6], pair_recv.at[6], s, other),
        remote(blend_ref, blend_in, pair_send.at[7], pair_recv.at[7], s, other),
        remote(weighed.at[c], weighed.at[c], pair_send.at[0], pair_recv.at[0], s, other),
        remote(gate_hbm.at[1 - c], gate_w.at[1], pair_send.at[2], pair_recv.at[2], s, other),
        remote(up_hbm.at[1 - c], up_w.at[1], pair_send.at[3], pair_recv.at[3], s, other),
        remote(down_hbm.at[1 - c], down_w.at[1], pair_send.at[4], pair_recv.at[4], s, other),
    ]
    for copy in pair:
        copy.start()

    first = matmul(mixed_ref[:, c].reshape(256, 256), blend_ref[...])
    pair[0].wait_recv()
    pair[1].wait_recv()
    both = first + matmul(mixed_in[...].reshape(256, 256), blend_in[...])
    projected[...] = both.astype(BF16).reshape(NZ, 2, 16, WIDTH)
    summed = ring_reduce(projected, landing4p, landing3p, project_send, project_recv, z, c, s)
    stream = (skip_ref[...].astype(F32) + jnp.concatenate(summed, axis=0)).astype(BF16)
    after[...] = stream
    stream = stream.astype(F32)
    scale = lax.rsqrt(jnp.mean(stream * stream, axis=-1, keepdims=True) + EPSILON)
    normed[...] = (stream * scale * gain_ref[...]).astype(BF16)
    tokens[c] = normed[...]
    swap = remote(normed, tokens.at[c], pair_send.at[1], pair_recv.at[1], s, other)
    swap.start()
    pair[2].wait_recv()
    swap.wait_recv()
    pair.append(swap)

    weight = weighed[...].reshape(64, 128)
    named = jnp.where(weight > 0.0, 1.0, 0.0)
    token_row = lax.broadcasted_iota(jnp.int32, (64, 64), 0)
    token_col = lax.broadcasted_iota(jnp.int32, (64, 64), 1)
    earlier = jnp.where(
        (token_col < token_row) & ((token_col >= 32) == (token_row >= 32)), 1.0, 0.0
    )
    rank = matmul(earlier.astype(BF16), named.astype(BF16))
    lane_e = lax.broadcasted_iota(jnp.int32, (128, 128), 0)
    slot_lane = lax.broadcasted_iota(jnp.int32, (128, 128), 1)
    spread = jnp.where(lane_e == 2 * (slot_lane // 8) + c, 1.0, 0.0)
    place = lax.rem(lax.broadcasted_iota(jnp.int32, (64, 128), 1), 8)
    second = jnp.where(place >= 3, 1, 0)
    token_core = jnp.where(lax.broadcasted_iota(jnp.int32, (64, 128), 0) >= 32, 1, 0)
    wanted = (place - 3 * second).astype(F32)
    named_slot = matmul(named.astype(BF16), spread.astype(BF16))
    rank_slot = matmul(rank.astype(BF16), spread.astype(BF16))
    chosen = (
        (named_slot > 0.5) & (jnp.abs(rank_slot - wanted) < 0.5) & (token_core == second)
        & (place < 6)
    )
    onehot = jnp.where(chosen, 1.0, 0.0)
    weight_slot = jnp.where(
        chosen, jnp.dot(weight, spread, precision=HIGH, preferred_element_type=F32), 0.0
    )
    everything = tokens[...].reshape(64, WIDTH)
    filled = matmul(onehot.T.astype(BF16), everything)
    slots[...] = filled.reshape(NS, 8, WIDTH).astype(BF16)

    def send_slots(k, carry):
        peer = lax.rem(s + k, NS)
        remote(slots.at[peer], arrived.at[s], sp_send.at[k], sp_recv.at[k], peer, t).start()
        return carry

    lax.fori_loop(1, NS, send_slots, 0)
    arrived[s] = slots[s]

    def await_slots(k, carry):
        remote(slots.at[s], arrived.at[s], sp_send.at[k], sp_recv.at[k], s, t).wait_recv()
        return carry

    lax.fori_loop(1, NS, await_slots, 0)

    dense_row = lax.broadcasted_iota(jnp.int32, (96, 128), 0)
    padded_row = lax.broadcasted_iota(jnp.int32, (96, 128), 1)
    dense = jnp.where(padded_row == 8 * (dense_row // 6) + lax.rem(dense_row, 6), 1.0, 0.0)
    padded = arrived[...].astype(F32).reshape(128, WIDTH).astype(BF16)
    packed = matmul(dense.astype(BF16), padded).astype(BF16)
    rows[z] = packed.reshape(2, 48, WIDTH)

    def hop(upward, half, k):
        chunk = wrap(z - k, NZ) if upward else lax.rem(z + k, NZ)
        sem = (0 if upward else 8) + 4 * half + k
        return remote(
            rows.at[chunk, half],
            rows.at[chunk, half],
            gather_send.at[sem],
            gather_recv.at[sem],
            s,
            up if upward else down,
        )

    def arrival(upward, half, k):
        chunk = wrap(z - k - 1, NZ) if upward else lax.rem(z + k + 1, NZ)
        sem = (0 if upward else 8) + 4 * half + k
        return remote(
            rows.at[chunk, half],
            rows.at[chunk, half],
            gather_send.at[sem],
            gather_recv.at[sem],
            s,
            up if upward else down,
        )

    for upward, half in ((True, 0), (False, 1), (True, 1), (False, 0)):
        hop(upward, half, 0).start()
    for load in loads:
        load.wait()
    for copy in pair[3:6]:
        copy.wait_recv()

    def step(i, carry):
        k = (i - 1) // 2

        @pl.when(lax.rem(i, 2) == 1)
        def _():
            for upward, half in ((True, 0), (False, 1)):
                arrival(upward, half, k).wait_recv()

                @pl.when(k < 3)
                def _():
                    hop(upward, half, k + 1).start()

            @pl.when(k < 3)
            def _():
                for upward, half in ((True, 1), (False, 0)):
                    arrival(upward, half, k).wait_recv()

                    @pl.when(k < 2)
                    def _():
                        hop(upward, half, k + 1).start()

        shift = (i + 1) // 2
        chunk = jnp.where(lax.rem(i, 2) == 1, wrap(z - shift, NZ), lax.rem(z + shift, NZ))
        x = rows[chunk].reshape(96, WIDTH)
        total = None
        for part in range(2):
            gate = matmul(x, gate_w[part])
            wide = matmul(x, up_w[part])
            hidden = (gate * jax.nn.sigmoid(gate) * wide).astype(BF16)
            piece = matmul(hidden, down_w[part])
            total = piece if total is None else total + piece
        results[chunk] = total.astype(BF16).reshape(2, 48, WIDTH)
        return carry

    lax.fori_loop(0, 8, step, 0)
    for upward in (True, False):
        for half in (0, 1):
            for k in range(4 if upward == (half == 0) else 3):
                hop(upward, half, k).wait_send()

    summed = ring_reduce(results, landing4, landing3, reduce_send, reduce_recv, z, c, s)

    def end_slots(k, carry):
        remote(slots.at[s], arrived.at[s], sp_send.at[k], sp_recv.at[k], s, t).wait_send()
        return carry

    lax.fori_loop(1, NS, end_slots, 0)
    for copy in pair:
        copy.wait_send()

    reduced = jnp.concatenate([part.astype(BF16) for part in summed], axis=0)
    opened = matmul(dense.T.astype(BF16), reduced)
    slots[...] = opened.reshape(NS, 8, WIDTH).astype(BF16)

    def send_back(k, carry):
        peer = lax.rem(s + k, NS)
        remote(slots.at[peer], back.at[s], back_send.at[k], back_recv.at[k], peer, t).start()
        return carry

    lax.fori_loop(1, NS, send_back, 0)
    back[s] = slots[s]

    def await_back(k, carry):
        remote(slots.at[s], back.at[s], back_send.at[k], back_recv.at[k], s, t).wait_recv()
        return carry

    lax.fori_loop(1, NS, await_back, 0)
    answers = back[...].astype(F32).reshape(128, WIDTH).astype(BF16)
    high = weight_slot.astype(BF16)
    low = (weight_slot - high.astype(F32)).astype(BF16)
    mixture = matmul(high, answers) + matmul(low, answers)
    contribution[...] = mixture.reshape(2, 32, WIDTH)
    swap = remote(contribution.at[1 - c], incoming, pair_send.at[5], pair_recv.at[5], s, other)
    swap.start()
    kept = contribution[c] + after[...].astype(F32)
    swap.wait_recv()
    out_ref[...] = (kept + incoming[...]).astype(BF16)
    swap.wait_send()

    def end_back(k, carry):
        remote(slots.at[s], back.at[s], back_send.at[k], back_recv.at[k], s, t).wait_send()
        return carry

    lax.fori_loop(1, NS, end_back, 0)


def finish_layer(mixed, blend, skip, gain, picks, affinity, gate, up, down):
    vmem = pl.BlockSpec(memory_space=pltpu.VMEM)
    hbm = pl.BlockSpec(memory_space=pl.ANY)
    dma = pltpu.SemaphoreType.DMA
    return pl.pallas_call(
        moe_kernel,
        out_shape=jax.ShapeDtypeStruct((32, WIDTH), BF16),
        in_specs=[vmem] * 6 + [hbm] * 3,
        out_specs=vmem,
        scratch_shapes=[
            pltpu.VMEM((NZ, 32, 256), BF16),
            pltpu.VMEM((256, WIDTH), BF16),
            pltpu.VMEM((NZ, 2, 16, WIDTH), BF16),
            pltpu.VMEM((2, 4, 16, WIDTH), BF16),
            pltpu.VMEM((2, 3, 16, WIDTH), BF16),
            pltpu.VMEM((32, WIDTH), BF16),
            pltpu.VMEM((32, WIDTH), BF16),
            pltpu.VMEM((2, 32, WIDTH), BF16),
            pltpu.VMEM((2, 32, 128), F32),
            pltpu.VMEM((2, WIDTH, 256), BF16),
            pltpu.VMEM((2, WIDTH, 256), BF16),
            pltpu.VMEM((2, 256, WIDTH), BF16),
            pltpu.VMEM((NS, 8, WIDTH), BF16),
            pltpu.VMEM((NS, 8, WIDTH), BF16),
            pltpu.VMEM((NS, 8, WIDTH), BF16),
            pltpu.VMEM((NZ, 2, 48, WIDTH), BF16),
            pltpu.VMEM((NZ, 2, 48, WIDTH), BF16),
            pltpu.VMEM((2, 4, 48, WIDTH), BF16),
            pltpu.VMEM((2, 3, 48, WIDTH), BF16),
            pltpu.VMEM((2, 32, WIDTH), F32),
            pltpu.VMEM((32, WIDTH), F32),
            dma((3,)),
            dma((8,)),
            dma((8,)),
            dma((NS,)),
            dma((NS,)),
            dma((16,)),
            dma((16,)),
            dma((16,)),
            dma((16,)),
            dma((16,)),
            dma((16,)),
            dma((NS,)),
            dma((NS,)),
        ],
        compiler_params=pltpu.CompilerParams(
            collective_id=0, has_side_effects=True, vmem_limit_bytes=56 * 1024 * 1024
        ),
    )(
        mixed.reshape(NZ, 2, 32, 256),
        blend,
        skip,
        gain.reshape(1, WIDTH),
        picks,
        affinity,
        gate,
        up,
        down,
    )


def over_lanes(columns, direction):
    rows = columns.shape[0]
    low = lax.broadcasted_iota(jnp.int32, (rows, 128), 1) < HEAD_DIM
    pairs = []
    for pair in range(2):
        at = 4 * direction + 2 * pair
        pairs.append(jnp.where(low, columns[:, at : at + 1], columns[:, at + 1 : at + 2]))
    return jnp.concatenate(pairs, axis=1)


def mixer_kernel(
    feed_ref,
    write_ref,
    read_ref,
    feed_taps,
    write_taps,
    read_taps,
    raw_ref,
    fade_ref,
    extra_ref,
    switch_ref,
    gain_ref,
    out_ref,
    rim,
    padded,
    feed,
    write,
    read,
    decay_s,
    step_s,
    columns,
    states,
    mixed,
    ends_out,
    ends_in,
    totals_in,
    carry_out,
    carry_in,
    totals_out,
    rim_send,
    rim_recv,
    end_send,
    end_recv,
    total_send,
    total_recv,
    carry_send,
    carry_recv,
):
    s, t = lax.axis_index("sp"), lax.axis_index("tp")
    after_me, before_me = lax.rem(s + 1, NS), lax.rem(s + NS - 1, NS)
    greet((), True)

    spans = ((feed_ref, 0, 256), (write_ref, 256, 384), (read_ref, 384, 512))
    rims = []
    for k, (source, start, stop) in enumerate(spans):
        rims.append(
            remote(
                source.at[pl.ds(504, 8)],
                rim.at[0, :, start:stop],
                rim_send.at[k],
                rim_recv.at[k],
                after_me,
                t,
            )
        )
        rims.append(
            remote(
                source.at[pl.ds(0, 8)],
                rim.at[1, :, start:stop],
                rim_send.at[3 + k],
                rim_recv.at[3 + k],
                before_me,
                t,
            )
        )
    for copy in rims:
        copy.start()
    for source, start, stop in spans:
        padded[8:520, start:stop] = source[...].astype(F32)

    for direction in range(2):
        raw = raw_ref[direction].astype(F32)
        step = jnp.maximum(raw, 0.0) + jnp.log1p(jnp.exp(-jnp.abs(raw)))
        head = lax.broadcasted_iota(jnp.int32, (4, 512), 0)
        fade = jnp.zeros((4, 512), F32)
        for h in range(4):
            fade = jnp.where(head == h, fade_ref[direction, h], fade)
        step_s[4 * direction : 4 * direction + 4, :] = step
        decay_s[4 * direction : 4 * direction + 4, :] = extra_ref[direction] - step * jnp.exp(fade)

    row = lax.broadcasted_iota(jnp.int32, (BLOCK, BLOCK), 0)
    col = lax.broadcasted_iota(jnp.int32, (BLOCK, BLOCK), 1)
    upto = jnp.where(row <= col, 1.0, 0.0)
    onward = jnp.where(row >= col, 1.0, 0.0)
    forward_rows = lax.broadcasted_iota(jnp.int32, (8, BLOCK), 0) < 4
    forward_lanes = lax.broadcasted_iota(jnp.int32, (1, 8), 1) < 4
    totals = []
    for b in range(4):
        span = slice(b * BLOCK, (b + 1) * BLOCK)
        piece = decay_s[:, span]
        run = jnp.where(
            forward_rows,
            jnp.dot(piece, upto, precision=HIGH, preferred_element_type=F32),
            jnp.dot(piece, onward, precision=HIGH, preferred_element_type=F32),
        )
        decay_s[:, span] = run
        run_columns = run.T
        total = jnp.where(
            forward_lanes, run_columns[BLOCK - 1 : BLOCK, :], run_columns[0:1, :]
        )
        totals.append(total)
        columns[0, b] = run_columns
        columns[1, b] = jnp.exp(total - run_columns) * step_s[:, span].T

    for copy in rims:
        copy.wait_recv()
    padded[0:8, :] = jnp.where(s > 0, rim[0].astype(F32), 0.0)
    padded[520:528, :] = jnp.where(s < NS - 1, rim[1].astype(F32), 0.0)

    for b in range(4):
        span = slice(b * BLOCK, (b + 1) * BLOCK)
        for taps, start, stop in (
            (feed_taps, 0, 256),
            (write_taps, 256, 384),
            (read_taps, 384, 512),
        ):
            summed = None
            for offset in range(CONV_W):
                term = taps[offset : offset + 1, :].astype(F32) * padded[
                    b * BLOCK + 6 + offset : b * BLOCK + 6 + offset + BLOCK, start:stop
                ]
                summed = term if summed is None else summed + term
            summed = summed * jax.nn.sigmoid(summed)
            if start == 0:
                feed[span, :] = summed
            elif start == 256:
                write[span, :] = summed
            else:
                read[span, :] = summed.astype(BF16)

    for b in range(4):
        span = slice(b * BLOCK, (b + 1) * BLOCK)
        ends = columns[1, b]
        x = feed[span, :]
        scaled = jnp.concatenate([x * over_lanes(ends, 0), x * over_lanes(ends, 1)], axis=1)
        states[b] = matmul(write[span, :].T.astype(BF16), scaled.astype(BF16))
    final = []
    for direction in range(2):
        lanes = slice(256 * direction, 256 * direction + 256)
        entering = jnp.zeros((STATE, 256), F32)
        for b in (range(4), range(3, -1, -1))[direction]:
            own = states[b, :, lanes]
            states[b, :, lanes] = entering
            entering = entering * jnp.exp(over_lanes(totals[b], direction)) + own
        final.append(entering.reshape(NS, 8, 256))
    ends_out[...] = jnp.concatenate(final, axis=1).astype(BF16)
    whole = totals[0] + totals[1] + totals[2] + totals[3]
    totals_out[...] = jnp.zeros((8, 128), F32)
    for direction in range(2):
        flat = over_lanes(whole, direction)
        for pair in range(2):
            at = 2 * direction + pair
            totals_out[at : at + 1, :] = flat[:, 128 * pair : 128 * pair + 128]

    def send_ends(k, carry):
        peer = lax.rem(s + k, NS)
        remote(ends_out.at[peer], ends_in.at[s], end_send.at[k], end_recv.at[k], peer, t).start()
        remote(totals_out, totals_in.at[s], total_send.at[k], total_recv.at[k], peer, t).start()
        return carry

    lax.fori_loop(1, NS, send_ends, 0)
    ends_in[s] = ends_out[s]
    totals_in[s] = totals_out[...]

    def within(b):
        span = slice(b * BLOCK, (b + 1) * BLOCK)
        inner = lax.dot_general(
            read[span, :],
            write[span, :].astype(BF16),
            (((1,), (1,)), ((), ())),
            preferred_element_type=F32,
        )
        run, step, run_columns = decay_s[:, span], step_s[:, span], columns[0, b]
        low = col < HEAD_DIM
        for pair in range(2):
            x = feed[span, 128 * pair : 128 * pair + 128].astype(BF16)
            parts = []
            for h in (2 * pair, 2 * pair + 1):
                k = 4 + h
                onto = jnp.exp(
                    jnp.where(row >= col, run_columns[:, h : h + 1] - run[h : h + 1, :], -jnp.inf)
                ) * step[h : h + 1, :]
                back = jnp.exp(
                    jnp.where(row <= col, run_columns[:, k : k + 1] - run[k : k + 1, :], -jnp.inf)
                ) * step[k : k + 1, :]
                parts.append(matmul(((onto + back) * inner).astype(BF16), x))
            mixed[span, 128 * pair : 128 * pair + 128] = jnp.where(low, parts[0], parts[1])

    within(0)
    within(1)

    def await_ends(k, carry):
        remote(ends_out.at[s], ends_in.at[s], end_send.at[k], end_recv.at[k], s, t).wait_recv()
        remote(totals_out, totals_in.at[s], total_send.at[k], total_recv.at[k], s, t).wait_recv()
        return carry

    lax.fori_loop(1, NS, await_ends, 0)
    def total_of(p, direction):
        pairs = [totals_in[p, 2 * direction + k : 2 * direction + k + 1, :] for k in range(2)]
        return jnp.exp(jnp.concatenate(pairs, axis=1))

    running = jnp.zeros((8, 256), F32)
    for p in range(NS):
        carry_out[p, 0:8, :] = running.astype(BF16)
        running = running * total_of(p, 0) + ends_in[p, 0:8, :].astype(F32)
    running = jnp.zeros((8, 256), F32)
    for p in range(NS - 1, -1, -1):
        carry_out[p, 8:16, :] = running.astype(BF16)
        running = running * total_of(p, 1) + ends_in[p, 8:16, :].astype(F32)

    def send_carry(k, carry):
        peer = lax.rem(s + k, NS)
        remote(
            carry_out.at[peer], carry_in.at[s], carry_send.at[k], carry_recv.at[k], peer, t
        ).start()
        return carry

    lax.fori_loop(1, NS, send_carry, 0)
    carry_in[s] = carry_out[s]
    within(2)
    within(3)

    def await_carry(k, carry):
        remote(
            carry_out.at[s], carry_in.at[s], carry_send.at[k], carry_recv.at[k], s, t
        ).wait_recv()
        return carry

    lax.fori_loop(1, NS, await_carry, 0)
    carried = carry_in[...].astype(F32)
    carried = (carried[:, 0:8, :].reshape(STATE, 256), carried[:, 8:16, :].reshape(STATE, 256))
    ahead = (
        jnp.zeros((1, 8), F32),
        totals[0],
        totals[0] + totals[1],
        totals[0] + totals[1] + totals[2],
    )
    behind = (
        totals[1] + totals[2] + totals[3],
        totals[2] + totals[3],
        totals[3],
        jnp.zeros((1, 8), F32),
    )
    for b in range(4):
        span = slice(b * BLOCK, (b + 1) * BLOCK)
        entering = jnp.concatenate(
            [
                carried[0] * jnp.exp(over_lanes(ahead[b], 0)),
                carried[1] * jnp.exp(over_lanes(behind[b], 1)),
            ],
            axis=1,
        )
        readout = matmul(read[span, :], (states[b] + entering).astype(BF16))
        reach = jnp.exp(columns[0, b])
        total = (
            mixed[span, :]
            + readout[:, 0:256] * over_lanes(reach, 0)
            + readout[:, 256:512] * over_lanes(reach, 1)
        )
        switch = switch_ref[span, :].astype(F32)
        gated = total * (switch * jax.nn.sigmoid(switch))
        scale = lax.rsqrt(jnp.mean(gated * gated, axis=-1, keepdims=True) + EPSILON)
        out_ref[span, :] = (gated * scale * gain_ref[...]).astype(BF16)

    for copy in rims:
        copy.wait_send()

    def end_sends(k, carry):
        remote(ends_out.at[s], ends_in.at[s], end_send.at[k], end_recv.at[k], s, t).wait_send()
        remote(totals_out, totals_in.at[s], total_send.at[k], total_recv.at[k], s, t).wait_send()
        remote(
            carry_out.at[s], carry_in.at[s], carry_send.at[k], carry_recv.at[k], s, t
        ).wait_send()
        return carry

    lax.fori_loop(1, NS, end_sends, 0)


def mix(feed, write, read, taps, raw, fade, extra, switch, gain):
    vmem = pl.BlockSpec(memory_space=pltpu.VMEM)
    smem = pl.BlockSpec(memory_space=pltpu.SMEM)
    dma = pltpu.SemaphoreType.DMA
    return pl.pallas_call(
        mixer_kernel,
        out_shape=jax.ShapeDtypeStruct((512, 256), BF16),
        in_specs=[vmem] * 7 + [smem] + [vmem] * 3,
        out_specs=vmem,
        scratch_shapes=[
            pltpu.VMEM((2, 8, 512), BF16),
            pltpu.VMEM((528, 512), F32),
            pltpu.VMEM((512, 256), F32),
            pltpu.VMEM((512, 128), F32),
            pltpu.VMEM((512, 128), BF16),
            pltpu.VMEM((8, 512), F32),
            pltpu.VMEM((8, 512), F32),
            pltpu.VMEM((2, 4, 128, 8), F32),
            pltpu.VMEM((4, 128, 512), F32),
            pltpu.VMEM((512, 256), F32),
            pltpu.VMEM((NS, 16, 256), BF16),
            pltpu.VMEM((NS, 16, 256), BF16),
            pltpu.VMEM((NS, 8, 128), F32),
            pltpu.VMEM((NS, 16, 256), BF16),
            pltpu.VMEM((NS, 16, 256), BF16),
            pltpu.VMEM((8, 128), F32),
            dma((6,)),
            dma((6,)),
            dma((NS,)),
            dma((NS,)),
            dma((NS,)),
            dma((NS,)),
            dma((NS,)),
            dma((NS,)),
        ],
        compiler_params=pltpu.CompilerParams(
            collective_id=1, has_side_effects=True, vmem_limit_bytes=40 * 1024 * 1024
        ),
    )(feed, write, read, *taps, raw, fade, extra, switch, gain.reshape(1, 256))


def per_device(
    skip_stream_entry,
    result_switch_mapped,
    channel_feed_mapped,
    write_coefficient_mapped,
    emission_coefficient_mapped,
    channel_feed_taps,
    write_coefficient_taps,
    emission_coefficient_taps,
    raw_increments,
    channel_log_fade_speed,
    extra_log_fade,
    cluster_scaling_factor,
    blend_result_matrix,
    routing_scaling_factor,
    specialist_switch_matrix,
    specialist_widen_matrix,
    specialist_contract_matrix,
    picked_specialists,
    router_affinities,
):
    mixed_rows = mix(
        channel_feed_mapped,
        write_coefficient_mapped,
        emission_coefficient_mapped,
        (channel_feed_taps, write_coefficient_taps, emission_coefficient_taps),
        raw_increments,
        channel_log_fade_speed,
        extra_log_fade,
        result_switch_mapped,
        cluster_scaling_factor,
    )
    return finish_layer(
        mixed_rows,
        blend_result_matrix,
        skip_stream_entry,
        routing_scaling_factor,
        picked_specialists,
        router_affinities,
        specialist_switch_matrix,
        specialist_widen_matrix,
        specialist_contract_matrix,
    )


def solution(mesh):
    in_specs = (
        P(("sp", "tp"), None),
        P("sp", "tp"),
        P("sp", "tp"),
        P("sp", "tp"),
        P("sp", "tp"),
        P(None, "tp"),
        P(None, "tp"),
        P(None, "tp"),
        P(None, "tp", "sp"),
        P(None, "tp"),
        P(None, "tp", "sp"),
        P("tp"),
        P("tp", None),
        P(),
        P("sp", None, "tp"),
        P("sp", None, "tp"),
        P("sp", "tp", None),
        P(("sp", "tp"), None),
        P(("sp", "tp"), None),
    )
    out_specs = P(("sp", "tp"), None)
    return jax.shard_map(
        per_device, mesh=mesh, in_specs=in_specs, out_specs=out_specs, check_vma=False
    )
```
